128 devices in a mesh: sp: 16 (over z, x), tp: 8 (over y, core).
Axes of the slice: x: 4, y: 4, z: 4, core: 2. Of those that a mesh axis runs over, the one named last changes fastest.
Arguments:
- tokens: bfloat16 [16384, 4096], P(('sp', 'tp')), may hold values from -6 to 6
- norm_gain: float32 [4096], replicated, may hold values from 0.1 to 1.9
- q_down: bfloat16 [4096, 768], replicated, may hold values from -0.09375 to 0.09375
- kv_down: bfloat16 [4096, 512], replicated, may hold values from -0.09375 to 0.09375
- rope_down: bfloat16 [4096, 32], replicated, may hold values from -8 to 8
- q_gain: float32 [768], replicated, may hold values from 0.1 to 1.9
- kv_gain: float32 [512], replicated, may hold values from 0.1 to 1.9
- q_up: bfloat16 [768, 1536], P(None, 'tp'), may hold values from -0.21875 to 0.21875
- kv_up: bfloat16 [512, 2048], P(None, 'tp'), may hold values from -0.25 to 0.25
- out_weight: bfloat16 [1024, 4096], replicated, may hold values from -0.1875 to 0.1875
- out_gain: float32 [4096], replicated, may hold values from 0.1 to 1.9
Outputs:
- mixed: bfloat16 [16384, 4096], P(('sp', 'tp'))
The draws below stay inside these ranges and needn't reach their ends.
All inputs are finite; a program needn't handle non-finite values.
Results may differ from the reference program's by a relative error of at most 0.02.
The reference program's roundings to bfloat16 on the way (of `normed`, `q_lat`, `kv_lat`, `key_rot`, `query`, `keys_values` and `attended`) count: a program that leaves them out, or rounds other values in their place, can miss the bound.
Values may be sent and summed in bfloat16 or wider, within the bound.
No kernel may reach another device: no remote copies, remote signals or barrier semaphores. Data moves between devices by JAX's collectives and lax.ppermute only.
A program may use at most 128 MiB of HBM per device.

```python
import jax
import jax.numpy as jnp
from jax import lax

D = 4096
HEADS = 16
NOPE = 64
ROPE = 32
VDIM = 64
Q_RANK = 768
KV_RANK = 512
TOKENS = 16384


def draw_rope_down(key, part):
    base = jax.random.normal(key, (D, ROPE), jnp.float32) * D ** (-0.5)
    return jnp.clip(base, -8.0, 8.0).astype(jnp.bfloat16)


def block_scale(stream_key, extent, split, smallest, high):
    level, own = 1.0, jax.random.fold_in(stream_key, 6)
    for dim, parts in split:
        steps = jnp.exp(jax.random.uniform(jax.random.fold_in(own, dim), (parts,), jnp.float32, smallest / len(split), high / len(split)))
        level = level * jnp.repeat(steps, extent[dim] // parts).reshape([-1 if axis == dim else 1 for axis in range(len(extent))])
    return level


def normal_values(key, dims, spread, bound, shards=(), kind=jnp.bfloat16):
    array = spread * jax.random.normal(key, dims, jnp.float32)
    if shards:
        array = array * block_scale(key, dims, shards, -0.22, 0.18)
    return jnp.clip(array, -bound, bound).astype(kind)


def setup_inputs(seed: int = 0) -> dict:
    arg_keys = jax.random.split(jax.random.key(seed), 12)
    tokens = normal_values(arg_keys[0], (TOKENS, D), 1.0, 6.0, ((0, 128),))
    norm_gain = jnp.clip(1.0 + 0.18 * jax.random.normal(arg_keys[1], (D,), jnp.float32), 0.1, 1.9)
    q_down = normal_values(arg_keys[2], (D, Q_RANK), D ** -0.5, 0.09375)
    kv_down = normal_values(arg_keys[3], (D, KV_RANK), D ** -0.5, 0.09375)
    rope_down = draw_rope_down(jax.random.fold_in(arg_keys[11], 71), 0)
    q_gain = jnp.clip(1.0 + 0.18 * jax.random.normal(arg_keys[5], (Q_RANK,), jnp.float32), 0.1, 1.9)
    kv_gain = jnp.clip(1.0 + 0.18 * jax.random.normal(arg_keys[6], (KV_RANK,), jnp.float32), 0.1, 1.9)
    q_up = normal_values(arg_keys[7], (Q_RANK, HEADS * (NOPE + ROPE)), Q_RANK ** -0.5, 0.21875, ((1, 8),))
    kv_up = normal_values(arg_keys[8], (KV_RANK, HEADS * (NOPE + VDIM)), KV_RANK ** -0.5, 0.25, ((1, 8),))
    out_weight = normal_values(arg_keys[9], (HEADS * VDIM, D), (HEADS * VDIM) ** -0.5, 0.1875)
    out_gain = jnp.clip(1.0 + 0.18 * jax.random.normal(arg_keys[10], (D,), jnp.float32), 0.1, 1.9)
    return dict(tokens=tokens, norm_gain=norm_gain, q_down=q_down, kv_down=kv_down, rope_down=rope_down, q_gain=q_gain, kv_gain=kv_gain, q_up=q_up, kv_up=kv_up, out_weight=out_weight, out_gain=out_gain)


EPS = 1e-06
THETA = 500000.0

def scaled_norm(values_in, gain):
    values_in = values_in.astype(jnp.float32)
    return values_in * lax.rsqrt(lax.optimization_barrier(jnp.mean(values_in * values_in, axis=-1, keepdims=True)) + EPS) * gain.astype(jnp.float32)

def rotate(values_in, position):
    values_in = values_in.astype(jnp.float32)
    width = values_in.shape[-1]
    half_dim = width // 2
    inverse = 1.0 / THETA ** (jnp.arange(0, width, 2, dtype=jnp.float32) / width)
    angles = position[:, None] * inverse[None, :]
    angles = angles.reshape((angles.shape[0],) + (1,) * (values_in.ndim - 2) + (half_dim,))
    cosine = jnp.cos(angles)
    sine = jnp.sin(angles)
    left = values_in[..., :half_dim]
    right = values_in[..., half_dim:]
    return jnp.concatenate([left * cosine - right * sine, right * cosine + left * sine], axis=-1)

def reference(tokens, norm_gain, q_down, kv_down, rope_down, q_gain, kv_gain, q_up, kv_up, out_weight, out_gain):
    position = jnp.arange(TOKENS, dtype=jnp.float32)
    normed = scaled_norm(tokens, norm_gain).astype(jnp.bfloat16)
    q_lat = scaled_norm(jnp.dot(normed, q_down, preferred_element_type=jnp.float32), q_gain).astype(jnp.bfloat16)
    kv_lat = scaled_norm(jnp.dot(normed, kv_down, preferred_element_type=jnp.float32), kv_gain).astype(jnp.bfloat16)
    key_rot = rotate(jnp.dot(normed, rope_down, preferred_element_type=jnp.float32), position).astype(jnp.bfloat16)
    query = jnp.dot(q_lat, q_up, preferred_element_type=jnp.float32).reshape(TOKENS, HEADS, NOPE + ROPE)
    query = jnp.concatenate([query[..., :NOPE], rotate(query[..., NOPE:], position)], axis=-1).astype(jnp.bfloat16)
    keys_values = jnp.dot(kv_lat, kv_up, preferred_element_type=jnp.float32).astype(jnp.bfloat16)
    keys_values = keys_values.reshape(TOKENS, HEADS, NOPE + VDIM)
    key_nope = keys_values[..., :NOPE].astype(jnp.float32)
    values = keys_values[..., NOPE:].astype(jnp.float32)
    key_rot32 = key_rot.astype(jnp.float32)
    factor = (NOPE + ROPE) ** (-0.5)
    block_rows = 256 if TOKENS % 256 == 0 else TOKENS
    key_index = jnp.arange(TOKENS)

    def attend(index):
        first_row = index * block_rows
        query_block = lax.dynamic_slice_in_dim(query, first_row, block_rows, 0).astype(jnp.float32)
        scores = jnp.einsum('qhd,khd->hqk', query_block[..., :NOPE], key_nope)
        scores = (scores + jnp.einsum('qhd,kd->hqk', query_block[..., NOPE:], key_rot32)) * factor
        query_index = first_row + jnp.arange(block_rows)
        visible = key_index[None, :] <= query_index[:, None]
        scores = jnp.where(visible[None], scores, -1e+30)
        top_score = lax.optimization_barrier(jnp.max(scores, axis=-1, keepdims=True))
        weights = jnp.where(visible[None], jnp.exp(scores - top_score), 0.0)
        total = lax.optimization_barrier(jnp.sum(weights, axis=-1))
        rounded = lax.optimization_barrier(weights.astype(jnp.bfloat16)).astype(jnp.float32)
        summed = jnp.einsum('hqk,khd->qhd', rounded, values)
        return (summed / total.T[:, :, None]).astype(jnp.bfloat16)
    attended = lax.map(attend, jnp.arange(TOKENS // block_rows)).reshape(TOKENS, HEADS * VDIM)
    projected = jnp.dot(attended, out_weight, preferred_element_type=jnp.float32)
    return scaled_norm(projected, out_gain).astype(jnp.bfloat16)
```

```python
import functools

import jax
import jax.numpy as jnp
from jax import lax
from jax.experimental import pallas as pl
from jax.experimental.pallas import tpu as pltpu
from jax.sharding import PartitionSpec as P

BF = jnp.bfloat16
F32 = jnp.float32
EPS = 1e-06
THETA = 500000.0
AXES = ("sp", "tp")
VM = pl.BlockSpec(memory_space=pltpu.VMEM)
SM = pl.BlockSpec(memory_space=pltpu.SMEM)


def pairs(move):
    out = []
    for i in range(128):
        sp, tp = i // 8, i % 8
        z, x, y, c = move(sp // 4, sp % 4, tp // 2, tp % 2)
        out.append((i, ((z % 4) * 4 + x % 4) * 8 + (y % 4) * 2 + c % 2))
    return out


def back(perm):
    return [(b, a) for a, b in perm]


ALONG_Y = [pairs(lambda z, x, y, c, k=k: (z, x, y + k, c)) for k in range(4)]
ALONG_Z = [pairs(lambda z, x, y, c, k=k: (z + k, x, y, c)) for k in range(4)]
ALONG_X = [pairs(lambda z, x, y, c, k=k: (z, x + k, y, c)) for k in range(4)]
QUERY = [pairs(lambda z, x, y, c, k=k: (z + k, x if z < 2 else 3 - x, y, c)) for k in range(4)]
CORE = pairs(lambda z, x, y, c: (z, x, y, c + 1))


def send(a, perm):
    return lax.ppermute(a, AXES, perm)


def normed_rows(v, gain):
    return v * lax.rsqrt(jnp.mean(v * v, axis=-1, keepdims=True) + EPS) * gain


def kv_down_kernel(tok, gain, kvd, rd, kvg, cos, sin, normed, out, acc, accr):
    i = pl.program_id(0)
    step = kvd.shape[0]

    @pl.when(i == 0)
    def _():
        normed[...] = normed_rows(tok[...].astype(F32), gain[...]).astype(BF)
        acc[...] = jnp.zeros(acc.shape, F32)
        accr[...] = jnp.zeros(accr.shape, F32)

    part = normed[:, pl.ds(i * step, step)]
    acc[...] += jnp.dot(part, kvd[...], preferred_element_type=F32)
    accr[...] += jnp.dot(part, rd[...], preferred_element_type=F32)

    @pl.when(i == pl.num_programs(0) - 1)
    def _():
        out[0:512, :] = normed_rows(acc[...], kvg[...]).T.astype(BF)
        r = accr[...].T
        left, right = r[0:16], r[16:32]
        out[512:528, :] = (left * cos[...] - right * sin[...]).astype(BF)
        out[528:544, :] = (right * cos[...] + left * sin[...]).astype(BF)


def kv_down_call(tok, gain, kvd, rd, kvg, cos, sin, steps=4):
    rows, d = tok.shape
    step = d // steps
    whole = lambda a: pl.BlockSpec(a.shape, lambda i: (0, 0))
    return pl.pallas_call(
        kv_down_kernel,
        grid=(steps,),
        out_shape=[jax.ShapeDtypeStruct((rows, d), BF), jax.ShapeDtypeStruct((544, rows), BF)],
        in_specs=[
            whole(tok),
            whole(gain),
            pl.BlockSpec((step, kvd.shape[1]), lambda i: (i, 0)),
            pl.BlockSpec((step, rd.shape[1]), lambda i: (i, 0)),
            whole(kvg),
            whole(cos),
            whole(sin),
        ],
        out_specs=[pl.BlockSpec((rows, d), lambda i: (0, 0)), pl.BlockSpec((544, rows), lambda i: (0, 0))],
        scratch_shapes=[pltpu.VMEM((rows, 512), F32), pltpu.VMEM((rows, 32), F32)],
        name="kv_down",
    )(tok, gain, kvd, rd, kvg, cos, sin)


def q_down_kernel(normed, qd, qg, out, acc):
    i = pl.program_id(0)
    step = qd.shape[0]

    @pl.when(i == 0)
    def _():
        acc[...] = jnp.zeros(acc.shape, F32)

    acc[...] += jnp.dot(normed[:, pl.ds(i * step, step)], qd[...], preferred_element_type=F32)

    @pl.when(i == pl.num_programs(0) - 1)
    def _():
        out[...] = normed_rows(acc[...], qg[...]).T.astype(BF)


def q_down_call(normed, qd, qg, steps=4):
    rows, d = normed.shape
    step = d // steps
    return pl.pallas_call(
        q_down_kernel,
        grid=(steps,),
        out_shape=jax.ShapeDtypeStruct((768, rows), BF),
        in_specs=[
            pl.BlockSpec((rows, d), lambda i: (0, 0)),
            pl.BlockSpec((step, 768), lambda i: (i, 0)),
            pl.BlockSpec((1, 768), lambda i: (0, 0)),
        ],
        out_specs=pl.BlockSpec((768, rows), lambda i: (0, 0)),
        scratch_shapes=[pltpu.VMEM((rows, 768), F32)],
        name="q_down",
    )(normed, qd, qg)


def kv_up_kernel(s, p0, p1, p2, p3, own, other, o0, o1, o2, o3, wt, full):
    z, c = s[1], s[4]
    wt[0:256, :] = own[...].T
    wt[256:512, :] = other[...].T
    lat = jnp.concatenate([p[0:512, :] for p in (p0, p1, p2, p3)], axis=1)
    rot = jnp.concatenate([p[512:544, :] for p in (p0, p1, p2, p3)], axis=1)
    full[...] = jnp.dot(wt[...], lat, preferred_element_type=F32).astype(BF)
    for k, o in enumerate((o0, o1, o2, o3)):
        at = ((z + k - 2 * c + 4) & 3) * 128
        o[0:64, :] = full[pl.ds(pl.multiple_of(at, 128), 64), :]
        o[64:96, :] = rot
        o[96:160, :] = full[pl.ds(pl.multiple_of(at + 64, 64), 64), :]


def kv_up_call(s, parts, own, other):
    return pl.pallas_call(
        kv_up_kernel,
        out_shape=[jax.ShapeDtypeStruct((160, 512), BF)] * 4,
        in_specs=[SM] + [VM] * 6,
        out_specs=[VM] * 4,
        scratch_shapes=[pltpu.VMEM((512, 512), BF), pltpu.VMEM((512, 512), BF)],
        name="kv_up",
    )(s, *parts, own, other)


def q_up_kernel(s, p0, p1, p2, p3, own, other, cos, sin, o0, o1, o2, o3, wt, full):
    z, c = s[1], s[4]
    wt[0:192, :] = own[...].T
    wt[192:384, :] = other[...].T
    lat = jnp.concatenate([p[...] for p in (p0, p1, p2, p3)], axis=1)
    full[...] = jnp.dot(wt[...], lat, preferred_element_type=F32)
    for k, o in enumerate((o0, o1, o2, o3)):
        at = ((z + k - 2 * c + 4) & 3) * 96
        o[0:64, :] = full[pl.ds(pl.multiple_of(at, 32), 64), :].astype(BF)
        left = full[pl.ds(pl.multiple_of(at + 64, 32), 16), :]
        right = full[pl.ds(pl.multiple_of(at + 80, 16), 16), :]
        o[64:80, :] = (left * cos[...] - right * sin[...]).astype(BF)
        o[80:96, :] = (right * cos[...] + left * sin[...]).astype(BF)


def q_up_call(s, parts, own, other, cos, sin):
    return pl.pallas_call(
        q_up_kernel,
        out_shape=[jax.ShapeDtypeStruct((96, 512), BF)] * 4,
        in_specs=[SM] + [VM] * 8,
        out_specs=[VM] * 4,
        scratch_shapes=[pltpu.VMEM((384, 768), BF), pltpu.VMEM((384, 512), F32)],
        name="q_up",
    )(s, *parts, own, other, cos, sin)


SCALE = 1.4426950408889634 / 96 ** 0.5
def attn_kernel(first, last, s_ref, *refs):
    q_refs, refs = refs[:4], refs[4:]
    if first:
        (a_ref, b_ref, *refs) = refs
    else:
        (a_ref, b_ref, m_in, acc_in, *refs) = refs
    if last:
        (*out_refs, m_ref, acc_ref, qs, ks, vs) = refs
    else:
        (m_ref, acc_ref, qs, ks, vs) = refs
    xk, z, x, y, c = (s_ref[i] for i in range(5))
    if first:
        m_ref[...] = jnp.full(m_ref.shape, -1e30, F32)
        acc_ref[...] = jnp.zeros(acc_ref.shape, F32)
    else:
        m_ref[...] = m_in[...]
        acc_ref[...] = acc_in[...]
    for k in range(4):
        q = q_refs[k][...].astype(F32) * SCALE
        hi = q.astype(BF)
        qs[k, 0:96, :] = hi
        qs[k, 96:192, :] = (q - hi.astype(F32)).astype(BF)
        for p, r in enumerate((a_ref, b_ref)):
            kt = r[pl.ds(160 * k, 96), :]
            ks[k, pl.ds(512 * p, 512), :] = jnp.concatenate([kt, kt], axis=0).T
            vs[k, 0:64, pl.ds(512 * p, 512)] = r[pl.ds(160 * k + 96, 64), :]
            row = lax.broadcasted_iota(jnp.int32, (16, 512), 0)
            vs[k, 64:80, pl.ds(512 * p, 512)] = jnp.where(row == 0, 1.0, 0.0).astype(BF)

    def block(kq, kk, diag):
        m_old = m_ref[kq]
        q = qs[kq]
        s = jnp.dot(ks[kk], q, preferred_element_type=F32)
        if diag:
            kr = lax.broadcasted_iota(jnp.int32, (1024, 512), 0)
            qr = lax.broadcasted_iota(jnp.int32, (1024, 512), 1)
            kb = (y - (kr >> 7)) & 3
            par = jnp.where(kr < 512, c, 1 - c)
            kpos = kb * 256 + par * 128 + (kr & 127)
            qpos = ((y - (qr >> 7)) & 3) * 256 + c * 128 + (qr & 127)
            s = jnp.where(kpos <= qpos, s, -1e30)
        m_new = jnp.maximum(m_old, jnp.max(s, axis=0, keepdims=True))
        p = jnp.exp2(s - m_new).astype(BF)
        alpha = jnp.exp2(m_old - m_new)
        o = jnp.dot(vs[kk], p, preferred_element_type=F32)
        acc_ref[kq] = acc_ref[kq] * alpha + o
        m_ref[kq] = m_new

    @pl.loop(0, 4)
    def _(kq):
        zq = (z - kq + 4) & 3
        xq = jnp.where(zq < 2, x, 3 - x)
        spq = 4 * zq + xq
        @pl.loop(0, 4)
        def _(kk):
            spk = 4 * ((z - kk + 4) & 3) + xk
            @pl.when(spk < spq)
            def _(): block(kq, kk, False)
            @pl.when(spk == spq)
            def _(): block(kq, kk, True)
    if last:
        for k in range(4):
            a = acc_ref[k]
            out_refs[k][...] = (a[0:64] / a[64:65]).astype(BF)

def attention(scal, q, a, b, state=None, last=False):
    first = state is None
    vm = pl.BlockSpec(memory_space=pltpu.VMEM)
    outs = [jax.ShapeDtypeStruct((4, 1, 512), F32), jax.ShapeDtypeStruct((4, 80, 512), F32)]
    if last: outs = [jax.ShapeDtypeStruct((64, 512), BF)] * 4 + outs
    args = (scal, *q, a, b) + (() if first else tuple(state))
    r = pl.pallas_call(functools.partial(attn_kernel, first, last), out_shape=outs,
        in_specs=[pl.BlockSpec(memory_space=pltpu.SMEM)] + [vm] * (len(args) - 1),
        out_specs=[vm] * len(outs),
        scratch_shapes=[pltpu.VMEM((4, 192, 512), BF), pltpu.VMEM((4, 1024, 192), BF), pltpu.VMEM((4, 80, 1024), BF)],
        compiler_params=pltpu.CompilerParams(vmem_limit_bytes=40 * 2**20), name="attn")(*args)
    return r


def out_kernel(s, t0, t1, t2, t3, w, gain, out, heads, rows, proj):
    i = pl.program_id(0)
    z, y = s[1], s[3]
    step = w.shape[1]

    @pl.when(i == 0)
    def _():
        for j, t in enumerate((t0, t1, t2, t3)):
            for k in range(4):
                at = (4 * ((y + j) & 3) + ((z + k) & 3)) * 64
                heads[pl.ds(pl.multiple_of(at, 64), 64), :] = t[pl.ds(64 * k, 64), :]
        rows[...] = heads[...].T

    proj[i] = jnp.dot(rows[...], w[...], preferred_element_type=F32)

    @pl.when(i == pl.num_programs(0) - 1)
    def _():
        steps = proj.shape[0]
        total = jnp.zeros((rows.shape[0], 1), F32)
        for n in range(steps):
            total += jnp.sum(proj[n] * proj[n], axis=-1, keepdims=True)
        scale = lax.rsqrt(total / (steps * step) + EPS)
        for n in range(steps):
            part = pl.ds(n * step, step)
            out[:, part] = (proj[n] * scale * gain[:, part]).astype(BF)


def out_call(s, parts, w, gain, steps=4):
    depth, d = w.shape
    step = d // steps
    return pl.pallas_call(
        out_kernel,
        grid=(steps,),
        out_shape=jax.ShapeDtypeStruct((128, d), BF),
        in_specs=[SM]
        + [pl.BlockSpec((256, 128), lambda i: (0, 0))] * 4
        + [pl.BlockSpec((depth, step), lambda i: (0, i)), pl.BlockSpec((1, d), lambda i: (0, 0))],
        out_specs=pl.BlockSpec((128, d), lambda i: (0, 0)),
        scratch_shapes=[
            pltpu.VMEM((depth, 128), BF),
            pltpu.VMEM((128, depth), BF),
            pltpu.VMEM((steps, 128, step), F32),
        ],
        name="out_proj",
    )(s, *parts, w, gain)


def turns(position):
    inverse = 1.0 / THETA ** (jnp.arange(0, 32, 2, dtype=F32) / 32)
    angles = inverse[:, None] * position.astype(F32)[None, :]
    return jnp.cos(angles), jnp.sin(angles)


def local(tokens, norm_gain, q_down, kv_down, rope_down, q_gain, kv_gain, q_up, kv_up, out_weight, out_gain):
    sp, tp = lax.axis_index("sp"), lax.axis_index("tp")
    z, x, y, c = sp // 4, sp % 4, tp // 2, tp % 2
    scal = lambda xk: jnp.stack([xk, z, x, y, c]).astype(jnp.int32)
    here = scal(x)
    lane = jnp.arange(128)
    cos_own, sin_own = turns((sp * 8 + tp) * 128 + lane)
    block = (y - jnp.arange(4)) % 4
    cos_q, sin_q = turns((sp * 1024 + block[:, None] * 256 + c * 128 + lane[None, :]).reshape(-1))

    kv_up_other = send(kv_up, CORE)
    q_up_other = send(q_up, CORE)
    normed, lat = kv_down_call(
        tokens, norm_gain[None], kv_down, rope_down, kv_gain[None], cos_own, sin_own
    )
    lats = [lat] + [send(lat, ALONG_Y[k]) for k in (1, 2, 3)]
    q_lat = q_down_call(normed, q_down, q_gain[None])
    q_lats = [q_lat] + [send(q_lat, ALONG_Y[k]) for k in (1, 2, 3)]

    kvs = kv_up_call(here, lats, kv_up, kv_up_other)
    mine = jnp.concatenate([kvs[0]] + [send(kvs[k], ALONG_Z[k]) for k in (1, 2, 3)], axis=0)
    qs = q_up_call(here, q_lats, q_up, q_up_other, cos_q, sin_q)
    qs = [send(qs[k], QUERY[k]) for k in range(4)]

    state = None
    for n, k in enumerate((0, 1, 3, 2)):
        a = mine if k == 0 else send(mine, ALONG_X[k])
        b = send(a, CORE)
        result = attention(scal((x - k) % 4), qs, a, b, state, last=n == 3)
        state = result[-2:]
    ret = jnp.concatenate([send(result[k], back(QUERY[k])) for k in range(4)], axis=0)
    parts = [ret[:, :128]] + [
        send(ret[:, 128 * j : 128 * j + 128], back(ALONG_Y[j])) for j in (1, 2, 3)
    ]
    return out_call(here, parts, out_weight, out_gain[None])


def solution(mesh):
    return jax.shard_map(
        local,
        mesh=mesh,
        in_specs=(
            P(AXES, None),
            P(),
            P(),
            P(),
            P(),
            P(),
            P(),
            P(None, "tp"),
            P(None, "tp"),
            P(),
            P(),
        ),
        out_specs=P(AXES, None),
        check_vma=False,
    )
```

```python
import functools

import jax
import jax.numpy as jnp
from jax import lax
from jax.experimental import pallas as pl
from jax.experimental.pallas import tpu as pltpu
from jax.sharding import PartitionSpec as P


BF = jnp.bfloat16
F32 = jnp.float32
EPS = 1e-06
THETA = 500000.0
AXES = ("sp", "tp")
VM = pl.BlockSpec(memory_space=pltpu.VMEM)
SM = pl.BlockSpec(memory_space=pltpu.SMEM)


PER_US = 3e8


def small(mib):
    return pltpu.CompilerParams(vmem_limit_bytes=mib * 2**20)


def pairs(move):
    out = []
    for i in range(128):
        sp, tp = i // 8, i % 8
        z, x, y, c = move(sp // 4, sp % 4, tp // 2, tp % 2)
        out.append((i, ((z % 4) * 4 + x % 4) * 8 + (y % 4) * 2 + c % 2))
    return out


def back(perm):
    return [(b, a) for a, b in perm]


ALONG_Y = [pairs(lambda z, x, y, c, k=k: (z, x, y + k, c)) for k in range(4)]
ALONG_Z = [pairs(lambda z, x, y, c, k=k: (z + k, x, y, c)) for k in range(4)]
ALONG_X = [pairs(lambda z, x, y, c, k=k: (z, x + k, y, c)) for k in range(4)]
CORE = pairs(lambda z, x, y, c: (z, x, y, c + 1))


def send(a, perm):
    return lax.ppermute(a, AXES, perm)


def normed_rows(v, gain):
    return v * lax.rsqrt(jnp.mean(v * v, axis=-1, keepdims=True) + EPS) * gain


CHUNKS = 4


def down_kernel(
    tok, gain, kvd, rd, kvg, qd, qg, cos, sin, out,
    tok_v, gain_v, kvd_v, rd_v, kvg_v, qd_v, qg_v, normed, sems,
):
    step = kvd.shape[0] // CHUNKS
    copies = {}

    def fetch(name, src, dst):
        copies[name] = pltpu.make_async_copy(src, dst, sems.at[len(copies)])
        copies[name].start()

    fetch("tok", tok, tok_v)
    fetch("gain", gain, gain_v)
    fetch("rd", rd, rd_v)
    for n in range(CHUNKS):
        fetch(("kv", n), kvd.at[pl.ds(n * step, step)], kvd_v.at[n])
    fetch("kvg", kvg, kvg_v)
    for n in range(CHUNKS):
        fetch(("q", n), qd.at[pl.ds(n * step, step)], qd_v.at[n])
    fetch("qg", qg, qg_v)
    copies["tok"].wait()
    copies["gain"].wait()
    normed[...] = normed_rows(tok_v[...].astype(F32), gain_v[...]).astype(BF)
    copies["rd"].wait()
    r = lax.dot_general(
        rd_v[...], normed[...], (((1,), (1,)), ((), ())), preferred_element_type=F32
    )
    left, right = r[0:16], r[16:32]
    out[512:528, :] = (left * cos[...] - right * sin[...]).astype(BF)
    out[528:544, :] = (right * cos[...] + left * sin[...]).astype(BF)

    def product(name, weights):
        total = None
        for n in range(CHUNKS):
            copies[(name, n)].wait()
            part = jnp.dot(
                normed[:, n * step : n * step + step], weights[n], preferred_element_type=F32
            )
            total = part if total is None else total + part
        return total

    total = product("kv", kvd_v)
    copies["kvg"].wait()
    out[0:512, :] = normed_rows(total, kvg_v[...]).T.astype(BF)
    total = product("q", qd_v)
    copies["qg"].wait()
    gain_q = jnp.concatenate([qg_v[n : n + 1, :] for n in range(6)], axis=1)
    out[544:1312, :] = normed_rows(total, gain_q).T.astype(BF)


def down_call(tok, gain, kvd, rd, kvg, qd, qg, cos, sin):
    rows, d = tok.shape
    step = d // CHUNKS
    return pl.pallas_call(
        down_kernel,
        out_shape=jax.ShapeDtypeStruct((1312, rows), BF),
        in_specs=[pl.BlockSpec(memory_space=pl.ANY)] * 7 + [VM] * 2,
        out_specs=VM,
        scratch_shapes=[
            pltpu.VMEM((rows, d), BF),
            pltpu.VMEM((1, d), F32),
            pltpu.VMEM((CHUNKS, step, 512), BF),
            pltpu.VMEM((32, d), BF),
            pltpu.VMEM((1, 512), F32),
            pltpu.VMEM((CHUNKS, step, 768), BF),
            pltpu.VMEM((6, 128), F32),
            pltpu.VMEM((rows, d), BF),
            pltpu.SemaphoreType.DMA((5 + 2 * CHUNKS,)),
        ],
        name="down",
    )(tok, gain, kvd, rd, kvg, qd, qg, cos, sin)


def up_kernel(
    s, p0, p1, p2, p3, kv_own, kv_other, q_own, q_other, cos, sin,
    near, q0, m1, m2, m3, kv_w, q_w, kv, q,
):
    z, c = s[1], s[4]
    parts = (p0, p1, p2, p3)
    kv_w[0:256, :] = kv_own[...].T
    kv_w[256:512, :] = kv_other[...].T
    q_w[0:192, :] = q_own[...]
    q_w[192:384, :] = q_other[...]
    lat = jnp.concatenate([p[0:512, :] for p in parts], axis=1)
    rot = jnp.concatenate([p[512:544, :] for p in parts], axis=1)
    kv[...] = jnp.dot(kv_w[...], lat, preferred_element_type=F32).astype(BF)
    lat = jnp.concatenate([p[544:1312, :] for p in parts], axis=1)
    q[...] = jnp.dot(q_w[...], lat, preferred_element_type=F32)
    for k, out in enumerate((None, m1, m2, m3)):
        head = (z + k - 2 * c + 4) & 3
        at = head * 128
        to = near if k == 0 else out
        to[0:64, :] = kv[pl.ds(pl.multiple_of(at, 128), 64), :]
        to[64:96, :] = rot
        to[96:160, :] = kv[pl.ds(pl.multiple_of(at + 64, 64), 64), :]
        to, low = (q0, 0) if k == 0 else (out, 160)
        at = head * 96
        left = q[pl.ds(pl.multiple_of(at + 64, 32), 16), :]
        right = q[pl.ds(pl.multiple_of(at + 80, 16), 16), :]
        to[low : low + 64, :] = q[pl.ds(pl.multiple_of(at, 32), 64), :].astype(BF)
        to[low + 64 : low + 80, :] = (left * cos[...] - right * sin[...]).astype(BF)
        to[low + 80 : low + 96, :] = (right * cos[...] + left * sin[...]).astype(BF)


def up_call(s, parts, *rest):
    piece = lambda rows: jax.ShapeDtypeStruct((rows, 512), BF)
    return pl.pallas_call(
        up_kernel,
        out_shape=[piece(160), piece(96)] + [piece(256)] * 3,
        in_specs=[SM] + [VM] * 10,
        out_specs=[VM] * 5,
        scratch_shapes=[
            pltpu.VMEM((512, 512), BF),
            pltpu.VMEM((384, 768), BF),
            pltpu.VMEM((512, 512), BF),
            pltpu.VMEM((384, 512), F32),
        ],
        compiler_params=small(16),
        name="up",
    )(s, *parts, *rest)


def gather_kernel(q0, m1, m2, m3, far, q):
    q[0:96, :] = q0[...]
    for n, m in enumerate((m1, m2, m3)):
        far[160 * n : 160 * n + 160, :] = m[0:160, :]
        q[96 * n + 96 : 96 * n + 192, :] = m[160:256, :]


def gather_call(*pieces):
    return pl.pallas_call(
        gather_kernel,
        out_shape=[jax.ShapeDtypeStruct((480, 512), BF), jax.ShapeDtypeStruct((384, 512), BF)],
        in_specs=[VM] * 4,
        out_specs=[VM] * 2,
        compiler_params=small(8),
        name="gather",
    )(*pieces)


def regroup_kernel(r0, r1, r2, r3, *outs):
    for j, o in enumerate(outs):
        for k, r in enumerate((r0, r1, r2, r3)):
            o[64 * k : 64 * k + 64, :] = r[:, 128 * j : 128 * j + 128]


def regroup_call(*pieces):
    return pl.pallas_call(
        regroup_kernel,
        out_shape=[jax.ShapeDtypeStruct((256, 128), BF)] * 4,
        in_specs=[VM] * 4,
        out_specs=[VM] * 4,
        compiler_params=small(8),
        name="regroup",
    )(*pieces)


SCALE = 1.4426950408889634 / 96**0.5
LIMIT = 60.0


def attn_kernel(first, last, s_ref, *refs):
    outs = ()
    if first:
        own, other, near, far, acc_ref, qs, ks, vs, top, m_ref = refs
    elif last:
        qs, near, far, acc_in, *outs, ks, vs, top, m_ref, acc_ref = refs
    else:
        qs, near, far, acc_in, acc_ref, ks, vs, top, m_ref = refs
    xk, z, x, y, c = (s_ref[i] for i in range(5))

    def reset():
        top[...] = jnp.full(top.shape, -1e30, F32)
        if first:
            m_ref[...] = jnp.full(m_ref.shape, -1e30, F32)
            acc_ref[...] = jnp.zeros(acc_ref.shape, F32)
        else:
            acc_ref[...] = acc_in[...]
            m_ref[...] = acc_in[:, 80:81, :]

    row = lax.broadcasted_iota(jnp.int32, (16, 512), 0)
    ones = jnp.where(row == 0, 1.0, 0.0).astype(BF)
    for k in range(4):
        if first:
            for h, v in enumerate((own, other)):
                q = v[96 * k : 96 * k + 96, :].astype(F32) * SCALE
                high = q.astype(BF)
                qs[k, 0:96, 512 * h : 512 * h + 512] = high
                qs[k, 96:192, 512 * h : 512 * h + 512] = (q - high.astype(F32)).astype(BF)
        r, at = (near, 0) if k == 0 else (far, 160 * (k - 1))
        kt = r[at : at + 96, :]
        ks[k] = jnp.concatenate([kt, kt], axis=0).T
        vs[k, 0:64, :] = r[at + 96 : at + 160, :]
        vs[k, 64:80, :] = ones

    def exact(kq, kk, free):
        m_old = m_ref[kq]
        s = jnp.dot(ks[kk], qs[kq], preferred_element_type=F32)
        kr = lax.broadcasted_iota(jnp.int32, (512, 1024), 0)
        qr = lax.broadcasted_iota(jnp.int32, (512, 1024), 1)
        kpos = ((y - (kr >> 7)) & 3) * 256 + c * 128 + (kr & 127)
        par = jnp.where(qr < 512, c, 1 - c)
        qpos = ((y - (qr >> 7)) & 3) * 256 + par * 128 + (qr & 127)
        s = jnp.where(kpos <= qpos + free, s, -1e30)
        m_new = jnp.maximum(m_old, jnp.max(s, axis=0, keepdims=True))
        p = jnp.exp2(s - m_new).astype(BF)
        o = jnp.dot(vs[kk], p, preferred_element_type=F32)
        acc_ref[kq, 0:80] = acc_ref[kq, 0:80] * jnp.exp2(m_old - m_new) + o
        m_ref[kq] = m_new

    def fast(kq, keys):
        m = m_ref[kq]
        q = qs[kq]
        peak, o = None, None
        for kk in keys:
            s = jnp.dot(ks[kk], q, preferred_element_type=F32)
            high = jnp.max(s.reshape(64, 8, 1024), axis=0)
            peak = high if peak is None else jnp.maximum(peak, high)
            p = jnp.exp2(s - m).astype(BF)
            d = jnp.dot(vs[kk], p, preferred_element_type=F32)
            o = d if o is None else o + d
        acc_ref[kq, 0:80] += o
        top[...] = jnp.maximum(top[...], peak - m)

    def walk(quick):
        @pl.loop(0, 4)
        def _(kq):
            zq = (z - kq + 4) & 3
            full = zq + jnp.where(xk < x, 1, 0)

            diag = jnp.where(xk == x, 1, 0)
            some = 1 if first else jnp.where(zq == 0, 1, 0)
            start = jnp.minimum(jnp.where(quick, some, full), full)

            @pl.loop(1 - diag, start + 1)
            def _(j):
                at = jnp.where(j == 0, zq, j - 1)
                exact(kq, (z - at + 4) & 3, jnp.where(j == 0, 0, 2048))

            count = full - start

            @pl.loop(0, count // 2)
            def _(j):
                fast(kq, [(z - start - 2 * j - n + 8) & 3 for n in (0, 1)])

            @pl.when(count % 2 == 1)
            def _():
                fast(kq, [(z - full + 5) & 3])

    def attempt(turn):
        reset()
        walk(turn == 0)
        over = jnp.logical_not(jnp.max(top[...]) <= LIMIT)
        return jnp.where(jnp.logical_and(over, turn == 0), 1, 2)

    lax.while_loop(lambda turn: turn < 2, attempt, jnp.int32(0))

    @pl.when(jnp.logical_not(jnp.max(top[...]) <= LIMIT))
    def _():
        reset()
        walk(False)

    if outs:
        for k in range(4):
            for h, o in enumerate(outs):
                o[k, 0:80, :] = acc_ref[k, 0:80, 512 * h : 512 * h + 512]
                o[k, 80:81, :] = m_ref[k, :, 512 * h : 512 * h + 512]
    else:
        acc_ref[:, 80:81, :] = m_ref[...]


def attention(scal, near, far, queries=None, state=None, last=False):
    first = state is None
    outs = [jax.ShapeDtypeStruct((4, 88, 1024), F32)]
    scratch = [
        pltpu.VMEM((4, 512, 192), BF),
        pltpu.VMEM((4, 80, 512), BF),
        pltpu.VMEM((8, 1024), F32),
        pltpu.VMEM((4, 1, 1024), F32),
    ]
    if first:
        outs.append(jax.ShapeDtypeStruct((4, 192, 1024), BF))
        args = (scal, *queries, near, far)
    else:
        args = (scal, queries, near, far, state)
    if last:
        outs = [jax.ShapeDtypeStruct((4, 88, 512), F32)] * 2
        scratch.append(pltpu.VMEM((4, 88, 1024), F32))
    return pl.pallas_call(
        functools.partial(attn_kernel, first, last),
        out_shape=outs,
        in_specs=[SM] + [VM] * (len(args) - 1),
        out_specs=[VM] * len(outs),
        scratch_shapes=scratch,
        compiler_params=small(28),
        cost_estimate=pl.CostEstimate(flops=int(5 * PER_US), transcendentals=0, bytes_accessed=2**20),
        name="attn",
    )(*args)


def merge_kernel(mine, theirs, *outs):
    for k in range(4):
        m1, m2 = mine[k, 80:81, :], theirs[k, 80:81, :]
        m = jnp.maximum(m1, m2)
        a = mine[k, 0:72, :] * jnp.exp2(m1 - m) + theirs[k, 0:72, :] * jnp.exp2(m2 - m)
        outs[k][...] = (a[0:64] / a[64:65]).astype(BF)


def merge_call(mine, theirs):
    return pl.pallas_call(
        merge_kernel,
        out_shape=[jax.ShapeDtypeStruct((64, 512), BF)] * 4,
        in_specs=[VM] * 2,
        out_specs=[VM] * 4,
        compiler_params=small(8),
        name="merge",
    )(mine, theirs)


def out_kernel(s, t0, t1, t2, t3, w, gain, out, heads):
    z, y = s[1], s[3]
    for j, t in enumerate((t0, t1, t2, t3)):
        for k in range(4):
            at = (4 * ((y + j) & 3) + ((z + k) & 3)) * 64
            heads[pl.ds(pl.multiple_of(at, 64), 64), :] = t[64 * k : 64 * k + 64, :]
    rows = heads[...].T
    proj = jnp.dot(rows, w[...], preferred_element_type=F32)
    out[...] = normed_rows(proj, gain[...]).astype(BF)


def out_call(s, parts, w, gain):
    return pl.pallas_call(
        out_kernel,
        out_shape=jax.ShapeDtypeStruct((128, w.shape[1]), BF),
        in_specs=[SM] + [VM] * 6,
        out_specs=VM,
        scratch_shapes=[pltpu.VMEM((w.shape[0], 128), BF)],
        compiler_params=small(24),
        name="out_proj",
    )(s, *parts, w, gain)


def turns(position):
    inverse = 1.0 / THETA ** (jnp.arange(0, 32, 2, dtype=F32) / 32)
    angles = inverse[:, None] * position.astype(F32)[None, :]
    return jnp.cos(angles), jnp.sin(angles)


def local(tokens, norm_gain, q_down, kv_down, rope_down, q_gain, kv_gain, q_up, kv_up, out_weight, out_gain):
    sp, tp = lax.axis_index("sp"), lax.axis_index("tp")
    z, x, y, c = sp // 4, sp % 4, tp // 2, tp % 2
    scal = lambda xk: jnp.stack([xk, z, x, y, c]).astype(jnp.int32)
    here = scal(x)
    lane = jnp.arange(128)
    cos_own, sin_own = turns((sp * 8 + tp) * 128 + lane)
    block = (y - jnp.arange(4)) % 4
    cos_q, sin_q = turns((sp * 1024 + block[:, None] * 256 + c * 128 + lane[None, :]).reshape(-1))

    def sends(arrays, perms):
        out = []
        for a, perm in zip(arrays, perms):
            out.append(send(a, perm))
        return out

    q_up = q_up.T
    kv_up_other, q_up_other = sends([kv_up, q_up], [CORE] * 2)
    lat = down_call(
        tokens, norm_gain[None], kv_down, rope_down.T, kv_gain[None], q_down,
        q_gain.reshape(6, 128), cos_own, sin_own,
    )
    lats = [lat] + sends([lat] * 3, ALONG_Y[1:])
    near, q0, *moved = up_call(here, lats, kv_up, kv_up_other, q_up, q_up_other, cos_q, sin_q)
    moved = sends(moved, ALONG_Z[1:])
    turn = [ALONG_X[1], ALONG_X[3], ALONG_X[2]]
    near = [near] + sends([near] * 3, turn)
    far, queries = gather_call(q0, *moved)
    (other,) = sends([queries], [CORE])
    far = [far] + sends([far] * 3, turn)

    acc, qs = attention(here, near[0], far[0], (queries, other))
    for n, k in ((1, 1), (2, 3)):
        (acc,) = attention(scal((x - k) % 4), near[n], far[n], qs, acc)
    mine, theirs = attention(scal((x - 2) % 4), near[3], far[3], qs, acc, last=True)
    (theirs,) = sends([theirs], [CORE])
    result = merge_call(mine, theirs)
    ret = [result[0]] + sends(result[1:], [back(p) for p in ALONG_Z[1:]])
    parts = regroup_call(*ret)
    parts = [parts[0]] + sends(parts[1:], [back(p) for p in ALONG_Y[1:]])
    return out_call(here, parts, out_weight, out_gain[None])


def solution(mesh):
    return jax.shard_map(
        local,
        mesh=mesh,
        in_specs=(
            P(AXES, None),
            P(),
            P(),
            P(),
            P(),
            P(),
            P(),
            P(None, "tp"),
            P(None, "tp"),
            P(),
            P(),
        ),
        out_specs=P(AXES, None),
        check_vma=False,
    )
```

```python
import functools

import jax
import jax.numpy as jnp
from jax import lax
from jax.experimental import pallas as pl
from jax.experimental.pallas import tpu as pltpu
from jax.sharding import PartitionSpec as P


BF = jnp.bfloat16
F32 = jnp.float32
EPS = 1e-06
THETA = 500000.0
AXES = ("sp", "tp")
VM = pl.BlockSpec(memory_space=pltpu.VMEM)
SM = pl.BlockSpec(memory_space=pltpu.SMEM)


PER_US = 3e8


def small(mib):
    return pltpu.CompilerParams(vmem_limit_bytes=mib * 2**20)


def pairs(move):
    out = []
    for i in range(128):
        sp, tp = i // 8, i % 8
        z, x, y, c = move(sp // 4, sp % 4, tp // 2, tp % 2)
        out.append((i, ((z % 4) * 4 + x % 4) * 8 + (y % 4) * 2 + c % 2))
    return out


def back(perm):
    return [(b, a) for a, b in perm]


ALONG_Y = [pairs(lambda z, x, y, c, k=k: (z, x, y + k, c)) for k in range(4)]
ALONG_Z = [pairs(lambda z, x, y, c, k=k: (z + k, x, y, c)) for k in range(4)]
ALONG_X = [pairs(lambda z, x, y, c, k=k: (z, x + k, y, c)) for k in range(4)]
CORE = pairs(lambda z, x, y, c: (z, x, y, c + 1))


def send(a, perm):
    return lax.ppermute(a, AXES, perm)


def normed_rows(v, gain):
    return v * lax.rsqrt(jnp.mean(v * v, axis=-1, keepdims=True) + EPS) * gain


CHUNKS = 4


def down_kernel(
    tok, gain, kvd, rd, kvg, qd, qg, cos, sin, out, q_out,
    tok_v, gain_v, kvd_v, rd_v, kvg_v, qd_v, qg_v, normed, sems,
):
    step = kvd.shape[0] // CHUNKS
    copies = {}

    def fetch(name, src, dst):
        copies[name] = pltpu.make_async_copy(src, dst, sems.at[len(copies)])
        copies[name].start()

    fetch("tok", tok, tok_v)
    fetch("gain", gain, gain_v)
    fetch("rd", rd, rd_v)
    for n in range(CHUNKS):
        fetch(("kv", n), kvd.at[pl.ds(n * step, step)], kvd_v.at[n])
    fetch("kvg", kvg, kvg_v)
    for n in range(CHUNKS):
        fetch(("q", n), qd.at[pl.ds(n * step, step)], qd_v.at[n])
    fetch("qg", qg, qg_v)
    copies["tok"].wait()
    copies["gain"].wait()
    normed[...] = normed_rows(tok_v[...].astype(F32), gain_v[...]).astype(BF)
    copies["rd"].wait()
    r = lax.dot_general(
        rd_v[...], normed[...], (((1,), (1,)), ((), ())), preferred_element_type=F32
    )
    left, right = r[0:16], r[16:32]
    out[512:528, :] = (left * cos[...] - right * sin[...]).astype(BF)
    out[528:544, :] = (right * cos[...] + left * sin[...]).astype(BF)

    def product(name, weights):
        total = None
        for n in range(CHUNKS):
            copies[(name, n)].wait()
            part = jnp.dot(
                normed[:, n * step : n * step + step], weights[n], preferred_element_type=F32
            )
            total = part if total is None else total + part
        return total

    total = product("kv", kvd_v)
    copies["kvg"].wait()
    out[0:512, :] = normed_rows(total, kvg_v[...]).T.astype(BF)
    total = product("q", qd_v)
    copies["qg"].wait()
    gain_q = jnp.concatenate([qg_v[n : n + 1, :] for n in range(6)], axis=1)
    q_out[...] = normed_rows(total, gain_q).T.astype(BF)


def down_call(tok, gain, kvd, rd, kvg, qd, qg, cos, sin):
    rows, d = tok.shape
    step = d // CHUNKS
    return pl.pallas_call(
        down_kernel,
        out_shape=[jax.ShapeDtypeStruct((544, rows), BF), jax.ShapeDtypeStruct((768, rows), BF)],
        in_specs=[pl.BlockSpec(memory_space=pl.ANY)] * 7 + [VM] * 2,
        out_specs=[VM] * 2,
        scratch_shapes=[
            pltpu.VMEM((rows, d), BF),
            pltpu.VMEM((1, d), F32),
            pltpu.VMEM((CHUNKS, step, 512), BF),
            pltpu.VMEM((32, d), BF),
            pltpu.VMEM((1, 512), F32),
            pltpu.VMEM((CHUNKS, step, 768), BF),
            pltpu.VMEM((6, 128), F32),
            pltpu.VMEM((rows, d), BF),
            pltpu.SemaphoreType.DMA((5 + 2 * CHUNKS,)),
        ],
        name="down",
    )(tok, gain, kvd, rd, kvg, qd, qg, cos, sin)


def kv_up_kernel(s, p0, p1, p2, p3, own, other, o0, o1, o2, o3, w, kv):
    z, c = s[1], s[4]
    parts = (p0, p1, p2, p3)
    w[0:256, :] = own[...].T
    w[256:512, :] = other[...].T
    lat = jnp.concatenate([p[0:512, :] for p in parts], axis=1)
    rot = jnp.concatenate([p[512:544, :] for p in parts], axis=1)
    kv[...] = jnp.dot(w[...], lat, preferred_element_type=F32).astype(BF)
    for k, to in enumerate((o0, o1, o2, o3)):
        at = ((z + k - 2 * c + 4) & 3) * 128
        to[0:64, :] = kv[pl.ds(pl.multiple_of(at, 128), 64), :]
        to[64:96, :] = rot
        to[96:160, :] = kv[pl.ds(pl.multiple_of(at + 64, 64), 64), :]


def kv_up_call(s, parts, own, other):
    return pl.pallas_call(
        kv_up_kernel,
        out_shape=[jax.ShapeDtypeStruct((160, 512), BF)] * 4,
        in_specs=[SM] + [VM] * 6,
        out_specs=[VM] * 4,
        scratch_shapes=[pltpu.VMEM((512, 512), BF)] * 2,
        compiler_params=small(8),
        name="kv_up",
    )(s, *parts, own, other)


def q_up_kernel(s, p0, p1, p2, p3, own, other, cos, sin, o0, o1, o2, o3, w, q):
    z, c = s[1], s[4]
    w[0:192, :] = own[...]
    w[192:384, :] = other[...]
    lat = jnp.concatenate([p[...] for p in (p0, p1, p2, p3)], axis=1)
    q[...] = jnp.dot(w[...], lat, preferred_element_type=F32)
    for k, to in enumerate((o0, o1, o2, o3)):
        at = ((z + k - 2 * c + 4) & 3) * 96
        left = q[pl.ds(pl.multiple_of(at + 64, 32), 16), :]
        right = q[pl.ds(pl.multiple_of(at + 80, 16), 16), :]
        to[0:64, :] = q[pl.ds(pl.multiple_of(at, 32), 64), :].astype(BF)
        to[64:80, :] = (left * cos[...] - right * sin[...]).astype(BF)
        to[80:96, :] = (right * cos[...] + left * sin[...]).astype(BF)


def q_up_call(s, parts, own, other, cos, sin):
    return pl.pallas_call(
        q_up_kernel,
        out_shape=[jax.ShapeDtypeStruct((96, 512), BF)] * 4,
        in_specs=[SM] + [VM] * 8,
        out_specs=[VM] * 4,
        scratch_shapes=[pltpu.VMEM((384, 768), BF), pltpu.VMEM((384, 512), F32)],
        compiler_params=small(10),
        name="q_up",
    )(s, *parts, own, other, cos, sin)


def join_kernel(*refs):
    at = 0
    for r in refs[:-1]:
        refs[-1][at : at + r.shape[0], :] = r[...]
        at += r.shape[0]


def join_call(*pieces):
    rows = sum(p.shape[0] for p in pieces)
    return pl.pallas_call(
        join_kernel,
        out_shape=jax.ShapeDtypeStruct((rows, 512), BF),
        in_specs=[VM] * len(pieces),
        out_specs=VM,
        compiler_params=small(8),
        name="join",
    )(*pieces)


def regroup_kernel(r0, r1, r2, r3, *outs):
    for j, o in enumerate(outs):
        for k, r in enumerate((r0, r1, r2, r3)):
            o[64 * k : 64 * k + 64, :] = r[:, 128 * j : 128 * j + 128]


def regroup_call(*pieces):
    return pl.pallas_call(
        regroup_kernel,
        out_shape=[jax.ShapeDtypeStruct((256, 128), BF)] * 4,
        in_specs=[VM] * 4,
        out_specs=[VM] * 4,
        compiler_params=small(8),
        name="regroup",
    )(*pieces)


SCALE = 1.4426950408889634 / 96**0.5
LIMIT = 60.0


def attn_kernel(first, last, s_ref, *refs):
    outs = ()
    if first:
        own, other, near, far, acc_ref, qs, ks, vs, top, m_ref = refs
    elif last:
        qs, near, far, acc_in, *outs, ks, vs, top, m_ref, acc_ref = refs
    else:
        qs, near, far, acc_in, acc_ref, ks, vs, top, m_ref = refs
    xk, z, x, y, c = (s_ref[i] for i in range(5))

    def reset():
        top[...] = jnp.full(top.shape, -1e30, F32)
        if first:
            m_ref[...] = jnp.full(m_ref.shape, -1e30, F32)
            acc_ref[...] = jnp.zeros(acc_ref.shape, F32)
        else:
            acc_ref[...] = acc_in[...]
            m_ref[...] = acc_in[:, 80:81, :]

    row = lax.broadcasted_iota(jnp.int32, (16, 512), 0)
    ones = jnp.where(row == 0, 1.0, 0.0).astype(BF)
    for k in range(4):
        if first:
            for h, v in enumerate((own, other)):
                qs[k, :, 512 * h : 512 * h + 512] = v[96 * k : 96 * k + 96, :]
        r, at = (near, 0) if k == 0 else (far, 160 * (k - 1))
        kt = r[at : at + 96, :]
        ks[k] = kt.T
        vs[k, 0:64, :] = r[at + 96 : at + 160, :]
        vs[k, 64:80, :] = ones

    def exact(kq, kk, free):
        m_old = m_ref[kq]
        s = jnp.dot(ks[kk], qs[kq], preferred_element_type=F32) * SCALE
        kr = lax.broadcasted_iota(jnp.int32, (512, 1024), 0)
        qr = lax.broadcasted_iota(jnp.int32, (512, 1024), 1)
        kpos = ((y - (kr >> 7)) & 3) * 256 + c * 128 + (kr & 127)
        par = jnp.where(qr < 512, c, 1 - c)
        qpos = ((y - (qr >> 7)) & 3) * 256 + par * 128 + (qr & 127)
        s = jnp.where(kpos <= qpos + free, s, -1e30)
        m_new = jnp.maximum(m_old, jnp.max(s, axis=0, keepdims=True))
        p = jnp.exp2(s - m_new).astype(BF)
        o = jnp.dot(vs[kk], p, preferred_element_type=F32)
        acc_ref[kq, 0:80] = acc_ref[kq, 0:80] * jnp.exp2(m_old - m_new) + o
        m_ref[kq] = m_new

    def fast(kq, keys):
        m = m_ref[kq]
        q = qs[kq]
        peak, o = None, None
        for kk in keys:
            s = jnp.dot(ks[kk], q, preferred_element_type=F32)
            high = jnp.max(s.reshape(64, 8, 1024), axis=0)
            peak = high if peak is None else jnp.maximum(peak, high)
            p = jnp.exp2(s * SCALE - m).astype(BF)
            d = jnp.dot(vs[kk], p, preferred_element_type=F32)
            o = d if o is None else o + d
        acc_ref[kq, 0:80] += o
        top[...] = jnp.maximum(top[...], peak * SCALE - m)

    def walk(quick):
        @pl.loop(0, 4)
        def _(kq):
            zq = (z - kq + 4) & 3
            full = zq + jnp.where(xk < x, 1, 0)

            diag = jnp.where(xk == x, 1, 0)
            some = 0 if first else jnp.where(zq == 0, 1, 0)
            if first:

                @pl.when(jnp.logical_and(quick, full > 0))
                def _():
                    s = jnp.dot(ks[z & 3, 0:128], qs[kq], preferred_element_type=F32) * SCALE
                    m_ref[kq] = jnp.max(s, axis=0, keepdims=True)

            start = jnp.minimum(jnp.where(quick, some, full), full)

            @pl.loop(1 - diag, start + 1)
            def _(j):
                at = jnp.where(j == 0, zq, j - 1)
                exact(kq, (z - at + 4) & 3, jnp.where(j == 0, 0, 2048))

            count = full - start

            @pl.loop(0, count // 2)
            def _(j):
                fast(kq, [(z - start - 2 * j - n + 8) & 3 for n in (0, 1)])

            @pl.when(count % 2 == 1)
            def _():
                fast(kq, [(z - full + 5) & 3])

    def attempt(turn):
        reset()
        walk(turn == 0)
        over = jnp.logical_not(jnp.max(top[...]) <= LIMIT)
        return jnp.where(jnp.logical_and(over, turn == 0), 1, 2)

    lax.while_loop(lambda turn: turn < 2, attempt, jnp.int32(0))

    @pl.when(jnp.logical_not(jnp.max(top[...]) <= LIMIT))
    def _():
        reset()
        walk(False)

    if outs:
        for k in range(4):
            for h, o in enumerate(outs):
                o[k, 0:80, :] = acc_ref[k, 0:80, 512 * h : 512 * h + 512]
                o[k, 80:81, :] = m_ref[k, :, 512 * h : 512 * h + 512]
    else:
        acc_ref[:, 80:81, :] = m_ref[...]


def attention(scal, near, far, queries=None, state=None, last=False):
    first = state is None
    outs = [jax.ShapeDtypeStruct((4, 88, 1024), F32)]
    scratch = [
        pltpu.VMEM((4, 512, 96), BF),
        pltpu.VMEM((4, 80, 512), BF),
        pltpu.VMEM((8, 1024), F32),
        pltpu.VMEM((4, 1, 1024), F32),
    ]
    if first:
        outs.append(jax.ShapeDtypeStruct((4, 96, 1024), BF))
        args = (scal, *queries, near, far)
    else:
        args = (scal, queries, near, far, state)
    if last:
        outs = [jax.ShapeDtypeStruct((4, 88, 512), F32)] * 2
        scratch.append(pltpu.VMEM((4, 88, 1024), F32))
    return pl.pallas_call(
        functools.partial(attn_kernel, first, last),
        out_shape=outs,
        in_specs=[SM] + [VM] * (len(args) - 1),
        out_specs=[VM] * len(outs),
        scratch_shapes=scratch,
        compiler_params=small(28),
        cost_estimate=pl.CostEstimate(flops=int(5 * PER_US), transcendentals=0, bytes_accessed=2**20),
        name="attn",
    )(*args)


def merge_kernel(mine, theirs, *outs):
    for k in range(4):
        m1, m2 = mine[k, 80:81, :], theirs[k, 80:81, :]
        m = jnp.maximum(m1, m2)
        a = mine[k, 0:72, :] * jnp.exp2(m1 - m) + theirs[k, 0:72, :] * jnp.exp2(m2 - m)
        outs[k][...] = (a[0:64] / a[64:65]).astype(BF)


def merge_call(mine, theirs):
    return pl.pallas_call(
        merge_kernel,
        out_shape=[jax.ShapeDtypeStruct((64, 512), BF)] * 4,
        in_specs=[VM] * 2,
        out_specs=[VM] * 4,
        compiler_params=small(8),
        name="merge",
    )(mine, theirs)


def out_kernel(s, t0, t1, t2, t3, w, gain, out, heads):
    z, y = s[1], s[3]
    for j, t in enumerate((t0, t1, t2, t3)):
        for k in range(4):
            at = (4 * ((y + j) & 3) + ((z + k) & 3)) * 64
            heads[pl.ds(pl.multiple_of(at, 64), 64), :] = t[64 * k : 64 * k + 64, :]
    rows = heads[...].T
    proj = jnp.dot(rows, w[...], preferred_element_type=F32)
    out[...] = normed_rows(proj, gain[...]).astype(BF)


def out_call(s, parts, w, gain):
    return pl.pallas_call(
        out_kernel,
        out_shape=jax.ShapeDtypeStruct((128, w.shape[1]), BF),
        in_specs=[SM] + [VM] * 6,
        out_specs=VM,
        scratch_shapes=[pltpu.VMEM((w.shape[0], 128), BF)],
        compiler_params=small(24),
        name="out_proj",
    )(s, *parts, w, gain)


def turns(position):
    inverse = 1.0 / THETA ** (jnp.arange(0, 32, 2, dtype=F32) / 32)
    angles = inverse[:, None] * position.astype(F32)[None, :]
    return jnp.cos(angles), jnp.sin(angles)


def local(tokens, norm_gain, q_down, kv_down, rope_down, q_gain, kv_gain, q_up, kv_up, out_weight, out_gain):
    sp, tp = lax.axis_index("sp"), lax.axis_index("tp")
    z, x, y, c = sp // 4, sp % 4, tp // 2, tp % 2
    scal = lambda xk: jnp.stack([xk, z, x, y, c]).astype(jnp.int32)
    here = scal(x)
    lane = jnp.arange(128)
    cos_own, sin_own = turns((sp * 8 + tp) * 128 + lane)
    block = (y - jnp.arange(4)) % 4
    cos_q, sin_q = turns((sp * 1024 + block[:, None] * 256 + c * 128 + lane[None, :]).reshape(-1))

    def sends(arrays, perms):
        out = []
        for a, perm in zip(arrays, perms):
            out.append(send(a, perm))
        return out

    q_up = q_up.T
    kv_up_other, q_up_other = sends([kv_up, q_up], [CORE] * 2)
    lat, q_lat = down_call(
        tokens, norm_gain[None], kv_down, rope_down.T, kv_gain[None], q_down,
        q_gain.reshape(6, 128), cos_own, sin_own,
    )
    lats = [lat] + sends([lat] * 3, ALONG_Y[1:])
    q_lats = [q_lat] + sends([q_lat] * 3, ALONG_Y[1:])
    near, *moved = kv_up_call(here, lats, kv_up, kv_up_other)
    moved = sends(moved, ALONG_Z[1:])
    q0, *q_moved = q_up_call(here, q_lats, q_up, q_up_other, cos_q, sin_q)
    q_moved = sends(q_moved, ALONG_Z[1:])
    turn = [ALONG_X[1], ALONG_X[3], ALONG_X[2]]
    near = [near] + sends([near] * 3, turn)
    far = join_call(*moved)
    far = [far] + sends([far] * 3, turn)
    queries = join_call(q0, *q_moved)
    (other,) = sends([queries], [CORE])

    acc, qs = attention(here, near[0], far[0], (queries, other))
    for n, k in ((1, 1), (2, 3)):
        (acc,) = attention(scal((x - k) % 4), near[n], far[n], qs, acc)
    mine, theirs = attention(scal((x - 2) % 4), near[3], far[3], qs, acc, last=True)
    (theirs,) = sends([theirs], [CORE])
    result = merge_call(mine, theirs)
    ret = [result[0]] + sends(result[1:], [back(p) for p in ALONG_Z[1:]])
    parts = regroup_call(*ret)
    parts = [parts[0]] + sends(parts[1:], [back(p) for p in ALONG_Y[1:]])
    return out_call(here, parts, out_weight, out_gain[None])


def solution(mesh):
    return jax.shard_map(
        local,
        mesh=mesh,
        in_specs=(
            P(AXES, None),
            P(),
            P(),
            P(),
            P(),
            P(),
            P(),
            P(None, "tp"),
            P(None, "tp"),
            P(),
            P(),
        ),
        out_specs=P(AXES, None),
        check_vma=False,
    )
```

```python
import functools

import jax
import jax.numpy as jnp
from jax import lax
from jax.experimental import pallas as pl
from jax.experimental.pallas import tpu as pltpu
from jax.sharding import PartitionSpec as P


BF = jnp.bfloat16
F32 = jnp.float32
EPS = 1e-06
THETA = 500000.0
AXES = ("sp", "tp")
VM = pl.BlockSpec(memory_space=pltpu.VMEM)
SM = pl.BlockSpec(memory_space=pltpu.SMEM)


PER_US = 3e8


def small(mib):
    return pltpu.CompilerParams(vmem_limit_bytes=mib * 2**20)


def pairs(move):
    out = []
    for i in range(128):
        sp, tp = i // 8, i % 8
        z, x, y, c = move(sp // 4, sp % 4, tp // 2, tp % 2)
        out.append((i, ((z % 4) * 4 + x % 4) * 8 + (y % 4) * 2 + c % 2))
    return out


def back(perm):
    return [(b, a) for a, b in perm]


ALONG_Y = [pairs(lambda z, x, y, c, k=k: (z, x, y + k, c)) for k in range(4)]
ALONG_Z = [pairs(lambda z, x, y, c, k=k: (z + k, x, y, c)) for k in range(4)]
ALONG_X = [pairs(lambda z, x, y, c, k=k: (z, x + k, y, c)) for k in range(4)]
CORE = pairs(lambda z, x, y, c: (z, x, y, c + 1))


def send(a, perm):
    return lax.ppermute(a, AXES, perm)


def normed_rows(v, gain):
    return v * lax.rsqrt(jnp.mean(v * v, axis=-1, keepdims=True) + EPS) * gain


CHUNKS = 4


def fetcher(sems):
    copies = {}

    def fetch(name, src, dst):
        copies[name] = pltpu.make_async_copy(src, dst, sems.at[len(copies)])
        copies[name].start()

    return copies, fetch


def product(copies, normed, weights):
    step = weights.shape[1]
    total = None
    for n in range(CHUNKS):
        copies[n].wait()
        part = jnp.dot(
            normed[:, n * step : n * step + step], weights[n], preferred_element_type=F32
        )
        total = part if total is None else total + part
    return total


def kv_down_kernel(
    tok, gain, kvd, rd, kvg, cos, sin, normed, out, tok_v, gain_v, kvd_v, rd_v, kvg_v, sems
):
    step = kvd.shape[0] // CHUNKS
    copies, fetch = fetcher(sems)
    fetch("tok", tok, tok_v)
    fetch("gain", gain, gain_v)
    for n in range(CHUNKS):
        fetch(n, kvd.at[pl.ds(n * step, step)], kvd_v.at[n])
    fetch("rd", rd, rd_v)
    fetch("kvg", kvg, kvg_v)
    copies["tok"].wait()
    copies["gain"].wait()
    normed[...] = normed_rows(tok_v[...].astype(F32), gain_v[...]).astype(BF)
    total = product(copies, normed, kvd_v)
    copies["kvg"].wait()
    out[0:512, :] = normed_rows(total, kvg_v[...]).T.astype(BF)
    copies["rd"].wait()
    r = lax.dot_general(
        rd_v[...], normed[...], (((1,), (1,)), ((), ())), preferred_element_type=F32
    )
    left, right = r[0:16], r[16:32]
    out[512:528, :] = (left * cos[...] - right * sin[...]).astype(BF)
    out[528:544, :] = (right * cos[...] + left * sin[...]).astype(BF)


def kv_down_call(tok, gain, kvd, rd, kvg, cos, sin):
    rows, d = tok.shape
    return pl.pallas_call(
        kv_down_kernel,
        out_shape=[jax.ShapeDtypeStruct((rows, d), BF), jax.ShapeDtypeStruct((544, rows), BF)],
        in_specs=[pl.BlockSpec(memory_space=pl.ANY)] * 5 + [VM] * 2,
        out_specs=[VM] * 2,
        scratch_shapes=[
            pltpu.VMEM((rows, d), BF),
            pltpu.VMEM((1, d), F32),
            pltpu.VMEM((CHUNKS, d // CHUNKS, 512), BF),
            pltpu.VMEM((32, d), BF),
            pltpu.VMEM((1, 512), F32),
            pltpu.SemaphoreType.DMA((4 + CHUNKS,)),
        ],
        name="kv_down",
    )(tok, gain, kvd, rd, kvg, cos, sin)


def q_down_kernel(src, qd, qg, out, normed, qd_v, qg_v, sems):
    step = qd.shape[0] // CHUNKS
    copies, fetch = fetcher(sems)
    fetch("in", src, normed)
    for n in range(CHUNKS):
        fetch(n, qd.at[pl.ds(n * step, step)], qd_v.at[n])
    fetch("gain", qg, qg_v)
    copies["in"].wait()
    total = product(copies, normed, qd_v)
    copies["gain"].wait()
    gain = jnp.concatenate([qg_v[n : n + 1, :] for n in range(6)], axis=1)
    out[...] = normed_rows(total, gain).T.astype(BF)


def q_down_call(normed, qd, qg):
    rows, d = normed.shape
    return pl.pallas_call(
        q_down_kernel,
        out_shape=jax.ShapeDtypeStruct((768, rows), BF),
        in_specs=[pl.BlockSpec(memory_space=pl.ANY)] * 3,
        out_specs=VM,
        scratch_shapes=[
            pltpu.VMEM((rows, d), BF),
            pltpu.VMEM((CHUNKS, d // CHUNKS, 768), BF),
            pltpu.VMEM((6, 128), F32),
            pltpu.SemaphoreType.DMA((2 + CHUNKS,)),
        ],
        name="q_down",
    )(normed, qd, qg)


def kv_up_kernel(s, p0, p1, p2, p3, own, other, o0, o1, o2, o3, w, kv):
    z, c = s[1], s[4]
    parts = (p0, p1, p2, p3)
    w[0:256, :] = own[...].T
    w[256:512, :] = other[...].T
    lat = jnp.concatenate([p[0:512, :] for p in parts], axis=1)
    rot = jnp.concatenate([p[512:544, :] for p in parts], axis=1)
    kv[...] = jnp.dot(w[...], lat, preferred_element_type=F32).astype(BF)
    for k, to in enumerate((o0, o1, o2, o3)):
        at = ((z + k - 2 * c + 4) & 3) * 128
        to[0:64, :] = kv[pl.ds(pl.multiple_of(at, 128), 64), :]
        to[64:96, :] = rot
        to[96:160, :] = kv[pl.ds(pl.multiple_of(at + 64, 64), 64), :]


def kv_up_call(s, parts, own, other):
    return pl.pallas_call(
        kv_up_kernel,
        out_shape=[jax.ShapeDtypeStruct((160, 512), BF)] * 4,
        in_specs=[SM] + [VM] * 6,
        out_specs=[VM] * 4,
        scratch_shapes=[pltpu.VMEM((512, 512), BF)] * 2,
        compiler_params=small(8),
        name="kv_up",
    )(s, *parts, own, other)


def q_up_kernel(s, p0, p1, p2, p3, own, other, cos, sin, o0, o1, o2, o3, w, q):
    z, c = s[1], s[4]
    w[0:192, :] = own[...]
    w[192:384, :] = other[...]
    lat = jnp.concatenate([p[...] for p in (p0, p1, p2, p3)], axis=1)
    q[...] = jnp.dot(w[...], lat, preferred_element_type=F32)
    for k, to in enumerate((o0, o1, o2, o3)):
        at = ((z + k - 2 * c + 4) & 3) * 96
        left = q[pl.ds(pl.multiple_of(at + 64, 32), 16), :]
        right = q[pl.ds(pl.multiple_of(at + 80, 16), 16), :]
        to[0:64, :] = q[pl.ds(pl.multiple_of(at, 32), 64), :].astype(BF)
        to[64:80, :] = (left * cos[...] - right * sin[...]).astype(BF)
        to[80:96, :] = (right * cos[...] + left * sin[...]).astype(BF)


def q_up_call(s, parts, own, other, cos, sin):
    return pl.pallas_call(
        q_up_kernel,
        out_shape=[jax.ShapeDtypeStruct((96, 512), BF)] * 4,
        in_specs=[SM] + [VM] * 8,
        out_specs=[VM] * 4,
        scratch_shapes=[pltpu.VMEM((384, 768), BF), pltpu.VMEM((384, 512), F32)],
        compiler_params=small(10),
        name="q_up",
    )(s, *parts, own, other, cos, sin)


def join_kernel(*refs):
    at = 0
    for r in refs[:-1]:
        refs[-1][at : at + r.shape[0], :] = r[...]
        at += r.shape[0]


def join_call(*pieces):
    rows = sum(p.shape[0] for p in pieces)
    return pl.pallas_call(
        join_kernel,
        out_shape=jax.ShapeDtypeStruct((rows, 512), BF),
        in_specs=[VM] * len(pieces),
        out_specs=VM,
        compiler_params=small(8),
        name="join",
    )(*pieces)


def regroup_kernel(r0, r1, r2, r3, *outs):
    for j, o in enumerate(outs):
        for k, r in enumerate((r0, r1, r2, r3)):
            o[64 * k : 64 * k + 64, :] = r[:, 128 * j : 128 * j + 128]


def regroup_call(*pieces):
    return pl.pallas_call(
        regroup_kernel,
        out_shape=[jax.ShapeDtypeStruct((256, 128), BF)] * 4,
        in_specs=[VM] * 4,
        out_specs=[VM] * 4,
        compiler_params=small(8),
        name="regroup",
    )(*pieces)


SCALE = 1.4426950408889634 / 96**0.5
LIMIT = 60.0


def attn_kernel(first, last, s_ref, *refs):
    outs = ()
    if first:
        own, other, near, far, acc_ref, qs, ks, vs, top, m_ref = refs
    elif last:
        qs, near, far, acc_in, *outs, ks, vs, top, m_ref, acc_ref = refs
    else:
        qs, near, far, acc_in, acc_ref, ks, vs, top, m_ref = refs
    xk, z, x, y, c = (s_ref[i] for i in range(5))

    def reset():
        top[...] = jnp.full(top.shape, -1e30, F32)
        if first:
            m_ref[...] = jnp.full(m_ref.shape, -1e30, F32)
            acc_ref[...] = jnp.zeros(acc_ref.shape, F32)
        else:
            acc_ref[...] = acc_in[...]
            m_ref[...] = acc_in[:, 80:81, :]

    row = lax.broadcasted_iota(jnp.int32, (16, 512), 0)
    ones = jnp.where(row == 0, 1.0, 0.0).astype(BF)
    for k in range(4):
        if first:
            for h, v in enumerate((own, other)):
                qs[k, :, 512 * h : 512 * h + 512] = v[96 * k : 96 * k + 96, :]
        r, at = (near, 0) if k == 0 else (far, 160 * (k - 1))
        kt = r[at : at + 96, :]
        ks[k] = kt.T
        vs[k, 0:64, :] = r[at + 96 : at + 160, :]
        vs[k, 64:80, :] = ones

    def exact(kq, kk, free):
        m_old = m_ref[kq]
        s = jnp.dot(ks[kk], qs[kq], preferred_element_type=F32) * SCALE
        kr = lax.broadcasted_iota(jnp.int32, (512, 1024), 0)
        qr = lax.broadcasted_iota(jnp.int32, (512, 1024), 1)
        kpos = ((y - (kr >> 7)) & 3) * 256 + c * 128 + (kr & 127)
        par = jnp.where(qr < 512, c, 1 - c)
        qpos = ((y - (qr >> 7)) & 3) * 256 + par * 128 + (qr & 127)
        s = jnp.where(kpos <= qpos + free, s, -1e30)
        m_new = jnp.maximum(m_old, jnp.max(s, axis=0, keepdims=True))
        p = jnp.exp2(s - m_new).astype(BF)
        o = jnp.dot(vs[kk], p, preferred_element_type=F32)
        acc_ref[kq, 0:80] = acc_ref[kq, 0:80] * jnp.exp2(m_old - m_new) + o
        m_ref[kq] = m_new

    def fast(kq, keys):
        m = m_ref[kq]
        q = qs[kq]
        peak, o = None, None
        for kk in keys:
            s = jnp.dot(ks[kk], q, preferred_element_type=F32)
            high = jnp.max(s.reshape(64, 8, 1024), axis=0)
            peak = high if peak is None else jnp.maximum(peak, high)
            p = jnp.exp2(s * SCALE - m).astype(BF)
            d = jnp.dot(vs[kk], p, preferred_element_type=F32)
            o = d if o is None else o + d
        acc_ref[kq, 0:80] += o
        top[...] = jnp.maximum(top[...], peak * SCALE - m)

    def walk(quick):
        @pl.loop(0, 4)
        def _(kq):
            zq = (z - kq + 4) & 3
            full = zq + jnp.where(xk < x, 1, 0)

            diag = jnp.where(xk == x, 1, 0)
            some = 0 if first else jnp.where(zq == 0, 1, 0)
            if first:

                @pl.when(jnp.logical_and(quick, full > 0))
                def _():
                    s = jnp.dot(ks[z & 3, 0:128], qs[kq], preferred_element_type=F32) * SCALE
                    m_ref[kq] = jnp.max(s, axis=0, keepdims=True)

            start = jnp.minimum(jnp.where(quick, some, full), full)

            @pl.loop(1 - diag, start + 1)
            def _(j):
                at = jnp.where(j == 0, zq, j - 1)
                exact(kq, (z - at + 4) & 3, jnp.where(j == 0, 0, 2048))

            count = full - start

            @pl.loop(0, count // 2)
            def _(j):
                fast(kq, [(z - start - 2 * j - n + 8) & 3 for n in (0, 1)])

            @pl.when(count % 2 == 1)
            def _():
                fast(kq, [(z - full + 5) & 3])

    def attempt(turn):
        reset()
        walk(turn == 0)
        over = jnp.logical_not(jnp.max(top[...]) <= LIMIT)
        return jnp.where(jnp.logical_and(over, turn == 0), 1, 2)

    lax.while_loop(lambda turn: turn < 2, attempt, jnp.int32(0))

    @pl.when(jnp.logical_not(jnp.max(top[...]) <= LIMIT))
    def _():
        reset()
        walk(False)

    if outs:
        for k in range(4):
            for h, o in enumerate(outs):
                o[k, 0:80, :] = acc_ref[k, 0:80, 512 * h : 512 * h + 512]
                o[k, 80:81, :] = m_ref[k, :, 512 * h : 512 * h + 512]
    else:
        acc_ref[:, 80:81, :] = m_ref[...]


def attention(scal, near, far, queries=None, state=None, last=False):
    first = state is None
    outs = [jax.ShapeDtypeStruct((4, 88, 1024), F32)]
    scratch = [
        pltpu.VMEM((4, 512, 96), BF),
        pltpu.VMEM((4, 80, 512), BF),
        pltpu.VMEM((8, 1024), F32),
        pltpu.VMEM((4, 1, 1024), F32),
    ]
    if first:
        outs.append(jax.ShapeDtypeStruct((4, 96, 1024), BF))
        args = (scal, *queries, near, far)
    else:
        args = (scal, queries, near, far, state)
    if last:
        outs = [jax.ShapeDtypeStruct((4, 88, 512), F32)] * 2
        scratch.append(pltpu.VMEM((4, 88, 1024), F32))
    return pl.pallas_call(
        functools.partial(attn_kernel, first, last),
        out_shape=outs,
        in_specs=[SM] + [VM] * (len(args) - 1),
        out_specs=[VM] * len(outs),
        scratch_shapes=scratch,
        compiler_params=small(28),
        cost_estimate=pl.CostEstimate(flops=int(5 * PER_US), transcendentals=0, bytes_accessed=2**20),
        name="attn",
    )(*args)


def merge_kernel(mine, theirs, *outs):
    for k in range(4):
        m1, m2 = mine[k, 80:81, :], theirs[k, 80:81, :]
        m = jnp.maximum(m1, m2)
        a = mine[k, 0:72, :] * jnp.exp2(m1 - m) + theirs[k, 0:72, :] * jnp.exp2(m2 - m)
        outs[k][...] = (a[0:64] / a[64:65]).astype(BF)


def merge_call(mine, theirs):
    return pl.pallas_call(
        merge_kernel,
        out_shape=[jax.ShapeDtypeStruct((64, 512), BF)] * 4,
        in_specs=[VM] * 2,
        out_specs=[VM] * 4,
        compiler_params=small(8),
        name="merge",
    )(mine, theirs)


def out_kernel(s, t0, t1, t2, t3, w, gain, out, heads):
    z, y = s[1], s[3]
    for j, t in enumerate((t0, t1, t2, t3)):
        for k in range(4):
            at = (4 * ((y + j) & 3) + ((z + k) & 3)) * 64
            heads[pl.ds(pl.multiple_of(at, 64), 64), :] = t[64 * k : 64 * k + 64, :]
    rows = heads[...].T
    proj = jnp.dot(rows, w[...], preferred_element_type=F32)
    out[...] = normed_rows(proj, gain[...]).astype(BF)


def out_call(s, parts, w, gain):
    return pl.pallas_call(
        out_kernel,
        out_shape=jax.ShapeDtypeStruct((128, w.shape[1]), BF),
        in_specs=[SM] + [VM] * 6,
        out_specs=VM,
        scratch_shapes=[pltpu.VMEM((w.shape[0], 128), BF)],
        compiler_params=small(24),
        name="out_proj",
    )(s, *parts, w, gain)


def turns(position):
    inverse = 1.0 / THETA ** (jnp.arange(0, 32, 2, dtype=F32) / 32)
    angles = inverse[:, None] * position.astype(F32)[None, :]
    return jnp.cos(angles), jnp.sin(angles)


def local(tokens, norm_gain, q_down, kv_down, rope_down, q_gain, kv_gain, q_up, kv_up, out_weight, out_gain):
    sp, tp = lax.axis_index("sp"), lax.axis_index("tp")
    z, x, y, c = sp // 4, sp % 4, tp // 2, tp % 2
    scal = lambda xk: jnp.stack([xk, z, x, y, c]).astype(jnp.int32)
    here = scal(x)
    lane = jnp.arange(128)
    cos_own, sin_own = turns((sp * 8 + tp) * 128 + lane)
    block = (y - jnp.arange(4)) % 4
    cos_q, sin_q = turns((sp * 1024 + block[:, None] * 256 + c * 128 + lane[None, :]).reshape(-1))

    def sends(arrays, perms):
        out = []
        for a, perm in zip(arrays, perms):
            out.append(send(a, perm))
        return out

    q_up = q_up.T
    kv_up_other, q_up_other = sends([kv_up, q_up], [CORE] * 2)
    normed, lat = kv_down_call(
        tokens, norm_gain[None], kv_down, rope_down.T, kv_gain[None], cos_own, sin_own
    )
    lats = [lat] + sends([lat] * 3, ALONG_Y[1:])
    q_lat = q_down_call(normed, q_down, q_gain.reshape(6, 128))
    q_lats = [q_lat] + sends([q_lat] * 3, ALONG_Y[1:])
    near, *moved = kv_up_call(here, lats, kv_up, kv_up_other)
    moved = sends(moved, ALONG_Z[1:])
    q0, *q_moved = q_up_call(here, q_lats, q_up, q_up_other, cos_q, sin_q)
    q_moved = sends(q_moved, ALONG_Z[1:])
    turn = [ALONG_X[1], ALONG_X[3], ALONG_X[2]]
    near = [near] + sends([near] * 3, turn)
    far = join_call(*moved)
    far = [far] + sends([far] * 3, turn)
    queries = join_call(q0, *q_moved)
    (other,) = sends([queries], [CORE])

    acc, qs = attention(here, near[0], far[0], (queries, other))
    for n, k in ((1, 1), (2, 3)):
        (acc,) = attention(scal((x - k) % 4), near[n], far[n], qs, acc)
    mine, theirs = attention(scal((x - 2) % 4), near[3], far[3], qs, acc, last=True)
    (theirs,) = sends([theirs], [CORE])
    result = merge_call(mine, theirs)
    ret = [result[0]] + sends(result[1:], [back(p) for p in ALONG_Z[1:]])
    parts = regroup_call(*ret)
    parts = [parts[0]] + sends(parts[1:], [back(p) for p in ALONG_Y[1:]])
    return out_call(here, parts, out_weight, out_gain[None])


def solution(mesh):
    return jax.shard_map(
        local,
        mesh=mesh,
        in_specs=(
            P(AXES, None),
            P(),
            P(),
            P(),
            P(),
            P(),
            P(),
            P(None, "tp"),
            P(None, "tp"),
            P(),
            P(),
        ),
        out_specs=P(AXES, None),
        check_vma=False,
    )
```

```python
import functools

import jax
import jax.numpy as jnp
from jax import lax
from jax.experimental import pallas as pl
from jax.experimental.pallas import tpu as pltpu
from jax.sharding import PartitionSpec as P


BF = jnp.bfloat16
F32 = jnp.float32
EPS = 1e-06
THETA = 500000.0
AXES = ("sp", "tp")
VM = pl.BlockSpec(memory_space=pltpu.VMEM)
SM = pl.BlockSpec(memory_space=pltpu.SMEM)


PER_US = 3e8


def small(mib):
    return pltpu.CompilerParams(vmem_limit_bytes=mib * 2**20)


def pairs(move):
    out = []
    for i in range(128):
        sp, tp = i // 8, i % 8
        z, x, y, c = move(sp // 4, sp % 4, tp // 2, tp % 2)
        out.append((i, ((z % 4) * 4 + x % 4) * 8 + (y % 4) * 2 + c % 2))
    return out


def back(perm):
    return [(b, a) for a, b in perm]


ALONG_Y = [pairs(lambda z, x, y, c, k=k: (z, x, y + k, c)) for k in range(4)]
ALONG_Z = [pairs(lambda z, x, y, c, k=k: (z + k, x, y, c)) for k in range(4)]
ALONG_X = [pairs(lambda z, x, y, c, k=k: (z, x + k, y, c)) for k in range(4)]
CORE = pairs(lambda z, x, y, c: (z, x, y, c + 1))


def send(a, perm):
    return lax.ppermute(a, AXES, perm)


def normed_rows(v, gain):
    return v * lax.rsqrt(jnp.mean(v * v, axis=-1, keepdims=True) + EPS) * gain


CHUNKS = 4


def fetcher(sems):
    copies = {}

    def fetch(name, src, dst):
        copies[name] = pltpu.make_async_copy(src, dst, sems.at[len(copies)])
        copies[name].start()

    return copies, fetch


def product(copies, normed, weights):
    step = weights.shape[1]
    total = None
    for n in range(CHUNKS):
        copies[n].wait()
        part = jnp.dot(
            normed[:, n * step : n * step + step], weights[n], preferred_element_type=F32
        )
        total = part if total is None else total + part
    return total


def kv_down_kernel(
    tok, gain, kvd, rd, kvg, cos, sin, normed, out, tok_v, gain_v, kvd_v, rd_v, kvg_v, sems
):
    step = kvd.shape[0] // CHUNKS
    copies, fetch = fetcher(sems)
    fetch("tok", tok, tok_v)
    fetch("gain", gain, gain_v)
    for n in range(CHUNKS):
        fetch(n, kvd.at[pl.ds(n * step, step)], kvd_v.at[n])
    fetch("rd", rd, rd_v)
    fetch("kvg", kvg, kvg_v)
    copies["tok"].wait()
    copies["gain"].wait()
    normed[...] = normed_rows(tok_v[...].astype(F32), gain_v[...]).astype(BF)
    total = product(copies, normed, kvd_v)
    copies["kvg"].wait()
    out[0:512, :] = normed_rows(total, kvg_v[...]).T.astype(BF)
    copies["rd"].wait()
    r = lax.dot_general(
        rd_v[...], normed[...], (((1,), (1,)), ((), ())), preferred_element_type=F32
    )
    left, right = r[0:16], r[16:32]
    out[512:528, :] = (left * cos[...] - right * sin[...]).astype(BF)
    out[528:544, :] = (right * cos[...] + left * sin[...]).astype(BF)


def kv_down_call(tok, gain, kvd, rd, kvg, cos, sin):
    rows, d = tok.shape
    return pl.pallas_call(
        kv_down_kernel,
        out_shape=[jax.ShapeDtypeStruct((rows, d), BF), jax.ShapeDtypeStruct((544, rows), BF)],
        in_specs=[pl.BlockSpec(memory_space=pl.ANY)] * 5 + [VM] * 2,
        out_specs=[VM] * 2,
        scratch_shapes=[
            pltpu.VMEM((rows, d), BF),
            pltpu.VMEM((1, d), F32),
            pltpu.VMEM((CHUNKS, d // CHUNKS, 512), BF),
            pltpu.VMEM((32, d), BF),
            pltpu.VMEM((1, 512), F32),
            pltpu.SemaphoreType.DMA((4 + CHUNKS,)),
        ],
        name="kv_down",
    )(tok, gain, kvd, rd, kvg, cos, sin)


def q_down_kernel(src, qd, qg, out, normed, qd_v, qg_v, sems):
    step = qd.shape[0] // CHUNKS
    copies, fetch = fetcher(sems)
    fetch("in", src, normed)
    for n in range(CHUNKS):
        fetch(n, qd.at[pl.ds(n * step, step)], qd_v.at[n])
    fetch("gain", qg, qg_v)
    copies["in"].wait()
    total = product(copies, normed, qd_v)
    copies["gain"].wait()
    gain = jnp.concatenate([qg_v[n : n + 1, :] for n in range(6)], axis=1)
    out[...] = normed_rows(total, gain).T.astype(BF)


def q_down_call(normed, qd, qg):
    rows, d = normed.shape
    return pl.pallas_call(
        q_down_kernel,
        out_shape=jax.ShapeDtypeStruct((768, rows), BF),
        in_specs=[pl.BlockSpec(memory_space=pl.ANY)] * 3,
        out_specs=VM,
        scratch_shapes=[
            pltpu.VMEM((rows, d), BF),
            pltpu.VMEM((CHUNKS, d // CHUNKS, 768), BF),
            pltpu.VMEM((6, 128), F32),
            pltpu.SemaphoreType.DMA((2 + CHUNKS,)),
        ],
        name="q_down",
    )(normed, qd, qg)


def kv_up_kernel(s, p0, p1, p2, p3, own, other, o0, o1, o2, o3, w, kv):
    z, c = s[1], s[4]
    parts = (p0, p1, p2, p3)
    w[0:256, :] = own[...].T
    w[256:512, :] = other[...].T
    lat = jnp.concatenate([p[0:512, :] for p in parts], axis=1)
    rot = jnp.concatenate([p[512:544, :] for p in parts], axis=1)
    kv[...] = jnp.dot(w[...], lat, preferred_element_type=F32).astype(BF)
    for k, to in enumerate((o0, o1, o2, o3)):
        at = ((z + k - 2 * c + 4) & 3) * 128
        to[0:64, :] = kv[pl.ds(pl.multiple_of(at, 128), 64), :]
        to[64:96, :] = rot
        to[96:160, :] = kv[pl.ds(pl.multiple_of(at + 64, 64), 64), :]


def kv_up_call(s, parts, own, other):
    return pl.pallas_call(
        kv_up_kernel,
        out_shape=[jax.ShapeDtypeStruct((160, 512), BF)] * 4,
        in_specs=[SM] + [VM] * 6,
        out_specs=[VM] * 4,
        scratch_shapes=[pltpu.VMEM((512, 512), BF)] * 2,
        compiler_params=small(8),
        name="kv_up",
    )(s, *parts, own, other)


def q_up_kernel(s, p0, p1, p2, p3, own, other, cos, sin, o0, o1, o2, o3, w, q):
    z, c = s[1], s[4]
    w[0:192, :] = own[...]
    w[192:384, :] = other[...]
    lat = jnp.concatenate([p[...] for p in (p0, p1, p2, p3)], axis=1)
    q[...] = jnp.dot(w[...], lat, preferred_element_type=F32)
    for k, to in enumerate((o0, o1, o2, o3)):
        at = ((z + k - 2 * c + 4) & 3) * 96
        left = q[pl.ds(pl.multiple_of(at + 64, 32), 16), :]
        right = q[pl.ds(pl.multiple_of(at + 80, 16), 16), :]
        to[0:64, :] = q[pl.ds(pl.multiple_of(at, 32), 64), :].astype(BF)
        to[64:80, :] = (left * cos[...] - right * sin[...]).astype(BF)
        to[80:96, :] = (right * cos[...] + left * sin[...]).astype(BF)


def q_up_call(s, parts, own, other, cos, sin):
    return pl.pallas_call(
        q_up_kernel,
        out_shape=[jax.ShapeDtypeStruct((96, 512), BF)] * 4,
        in_specs=[SM] + [VM] * 8,
        out_specs=[VM] * 4,
        scratch_shapes=[pltpu.VMEM((384, 768), BF), pltpu.VMEM((384, 512), F32)],
        compiler_params=small(10),
        name="q_up",
    )(s, *parts, own, other, cos, sin)


def join_kernel(*refs):
    at = 0
    for r in refs[:-1]:
        refs[-1][at : at + r.shape[0], :] = r[...]
        at += r.shape[0]


def join_call(*pieces):
    rows = sum(p.shape[0] for p in pieces)
    return pl.pallas_call(
        join_kernel,
        out_shape=jax.ShapeDtypeStruct((rows, 512), BF),
        in_specs=[VM] * len(pieces),
        out_specs=VM,
        compiler_params=small(8),
        name="join",
    )(*pieces)


def regroup_kernel(r0, r1, r2, r3, *outs):
    for j, o in enumerate(outs):
        for k, r in enumerate((r0, r1, r2, r3)):
            o[64 * k : 64 * k + 64, :] = r[:, 128 * j : 128 * j + 128]


def regroup_call(*pieces):
    return pl.pallas_call(
        regroup_kernel,
        out_shape=[jax.ShapeDtypeStruct((256, 128), BF)] * 4,
        in_specs=[VM] * 4,
        out_specs=[VM] * 4,
        compiler_params=small(8),
        name="regroup",
    )(*pieces)


SCALE = 1.4426950408889634 / 96**0.5
LIMIT = 60.0


def attn_kernel(first, last, s_ref, *refs):
    outs = ()
    if first:
        own, other, near, far, acc_ref, qs, ks, vs, top, m_ref = refs
    elif last:
        qs, near, far, acc_in, *outs, ks, vs, top, m_ref, acc_ref = refs
    else:
        qs, near, far, acc_in, acc_ref, ks, vs, top, m_ref = refs
    xk, z, x, y, c = (s_ref[i] for i in range(5))

    def reset():
        top[...] = jnp.full(top.shape, -1e30, F32)
        if first:
            m_ref[...] = jnp.full(m_ref.shape, -1e30, F32)
            acc_ref[...] = jnp.zeros(acc_ref.shape, F32)
        else:
            acc_ref[...] = acc_in[...]
            m_ref[...] = acc_in[:, 80:81, :]

    row = lax.broadcasted_iota(jnp.int32, (16, 512), 0)
    ones = jnp.where(row == 0, 1.0, 0.0).astype(BF)
    for k in range(4):
        if first:
            for h, v in enumerate((own, other)):
                qs[k, :, 512 * h : 512 * h + 512] = v[96 * k : 96 * k + 96, :]
        r, at = (near, 0) if k == 0 else (far, 160 * (k - 1))
        kt = r[at : at + 96, :]
        ks[k] = kt.T
        vs[k, 0:64, :] = r[at + 96 : at + 160, :]
        vs[k, 64:80, :] = ones

    def exact(kq, kk, free):
        m_old = m_ref[kq]
        s = jnp.dot(ks[kk], qs[kq], preferred_element_type=F32) * SCALE
        kr = lax.broadcasted_iota(jnp.int32, (512, 1), 0)
        qr = lax.broadcasted_iota(jnp.int32, (1, 1024), 1)
        kpos = ((y - (kr >> 7)) & 3) * 256 + c * 128 + (kr & 127)
        par = jnp.where(qr < 512, c, 1 - c)
        qpos = ((y - (qr >> 7)) & 3) * 256 + par * 128 + (qr & 127) + free
        s = jnp.where(kpos <= qpos, s, -1e30)
        m_new = jnp.maximum(m_old, jnp.max(s, axis=0, keepdims=True))
        p = jnp.exp2(s - m_new).astype(BF)
        o = jnp.dot(vs[kk], p, preferred_element_type=F32)
        acc_ref[kq, 0:80] = acc_ref[kq, 0:80] * jnp.exp2(m_old - m_new) + o
        m_ref[kq] = m_new

    def fast(kq, keys):
        m = m_ref[kq]
        q = qs[kq]
        peak, o = None, None
        for kk in keys:
            s = jnp.dot(ks[kk], q, preferred_element_type=F32)
            high = jnp.max(s.reshape(64, 8, 1024), axis=0)
            peak = high if peak is None else jnp.maximum(peak, high)
            p = jnp.exp2(s * SCALE - m).astype(BF)
            d = jnp.dot(vs[kk], p, preferred_element_type=F32)
            o = d if o is None else o + d
        acc_ref[kq, 0:80] += o
        top[...] = jnp.maximum(top[...], peak * SCALE - m)

    def walk(quick):
        @pl.loop(0, 4)
        def _(kq):
            zq = (z - kq + 4) & 3
            full = zq + jnp.where(xk < x, 1, 0)

            diag = jnp.where(xk == x, 1, 0)
            some = 0 if first else jnp.where(zq == 0, 1, 0)
            if first:

                @pl.when(jnp.logical_and(quick, full > 0))
                def _():
                    s = jnp.dot(ks[z & 3, 0:128], qs[kq], preferred_element_type=F32) * SCALE
                    m_ref[kq] = jnp.max(s, axis=0, keepdims=True)

            start = jnp.minimum(jnp.where(quick, some, full), full)

            @pl.loop(1 - diag, start + 1)
            def _(j):
                at = jnp.where(j == 0, zq, j - 1)
                exact(kq, (z - at + 4) & 3, jnp.where(j == 0, 0, 2048))

            count = full - start

            @pl.loop(0, count // 2)
            def _(j):
                fast(kq, [(z - start - 2 * j - n + 8) & 3 for n in (0, 1)])

            @pl.when(count % 2 == 1)
            def _():
                fast(kq, [(z - full + 5) & 3])

    def attempt(turn):
        reset()
        walk(turn == 0)
        over = jnp.logical_not(jnp.max(top[...]) <= LIMIT)
        return jnp.where(jnp.logical_and(over, turn == 0), 1, 2)

    lax.while_loop(lambda turn: turn < 2, attempt, jnp.int32(0))

    @pl.when(jnp.logical_not(jnp.max(top[...]) <= LIMIT))
    def _():
        reset()
        walk(False)

    if outs:
        for k in range(4):
            for h, o in enumerate(outs):
                o[k, 0:80, :] = acc_ref[k, 0:80, 512 * h : 512 * h + 512]
                o[k, 80:81, :] = m_ref[k, :, 512 * h : 512 * h + 512]
    else:
        acc_ref[:, 80:81, :] = m_ref[...]


def attention(scal, near, far, queries=None, state=None, last=False):
    first = state is None
    outs = [jax.ShapeDtypeStruct((4, 88, 1024), F32)]
    scratch = [
        pltpu.VMEM((4, 512, 96), BF),
        pltpu.VMEM((4, 80, 512), BF),
        pltpu.VMEM((8, 1024), F32),
        pltpu.VMEM((4, 1, 1024), F32),
    ]
    if first:
        outs.append(jax.ShapeDtypeStruct((4, 96, 1024), BF))
        args = (scal, *queries, near, far)
    else:
        args = (scal, queries, near, far, state)
    if last:
        outs = [jax.ShapeDtypeStruct((4, 88, 512), F32)] * 2
        scratch.append(pltpu.VMEM((4, 88, 1024), F32))
    return pl.pallas_call(
        functools.partial(attn_kernel, first, last),
        out_shape=outs,
        in_specs=[SM] + [VM] * (len(args) - 1),
        out_specs=[VM] * len(outs),
        scratch_shapes=scratch,
        compiler_params=small(28),
        cost_estimate=pl.CostEstimate(flops=int(5 * PER_US), transcendentals=0, bytes_accessed=2**20),
        name="attn",
    )(*args)


def merge_kernel(mine, theirs, *outs):
    for k in range(4):
        m1, m2 = mine[k, 80:81, :], theirs[k, 80:81, :]
        m = jnp.maximum(m1, m2)
        a = mine[k, 0:72, :] * jnp.exp2(m1 - m) + theirs[k, 0:72, :] * jnp.exp2(m2 - m)
        outs[k][...] = (a[0:64] / a[64:65]).astype(BF)


def merge_call(mine, theirs):
    return pl.pallas_call(
        merge_kernel,
        out_shape=[jax.ShapeDtypeStruct((64, 512), BF)] * 4,
        in_specs=[VM] * 2,
        out_specs=[VM] * 4,
        compiler_params=small(8),
        name="merge",
    )(mine, theirs)


def out_kernel(s, t0, t1, t2, t3, w, gain, out, heads):
    z, y = s[1], s[3]
    for j, t in enumerate((t0, t1, t2, t3)):
        for k in range(4):
            at = (4 * ((y + j) & 3) + ((z + k) & 3)) * 64
            heads[pl.ds(pl.multiple_of(at, 64), 64), :] = t[64 * k : 64 * k + 64, :]
    rows = heads[...].T
    proj = jnp.dot(rows, w[...], preferred_element_type=F32)
    out[...] = normed_rows(proj, gain[...]).astype(BF)


def out_call(s, parts, w, gain):
    return pl.pallas_call(
        out_kernel,
        out_shape=jax.ShapeDtypeStruct((128, w.shape[1]), BF),
        in_specs=[SM] + [VM] * 6,
        out_specs=VM,
        scratch_shapes=[pltpu.VMEM((w.shape[0], 128), BF)],
        compiler_params=small(24),
        name="out_proj",
    )(s, *parts, w, gain)


def turns(position):
    inverse = 1.0 / THETA ** (jnp.arange(0, 32, 2, dtype=F32) / 32)
    angles = inverse[:, None] * position.astype(F32)[None, :]
    return jnp.cos(angles), jnp.sin(angles)


def local(tokens, norm_gain, q_down, kv_down, rope_down, q_gain, kv_gain, q_up, kv_up, out_weight, out_gain):
    sp, tp = lax.axis_index("sp"), lax.axis_index("tp")
    z, x, y, c = sp // 4, sp % 4, tp // 2, tp % 2
    scal = lambda xk: jnp.stack([xk, z, x, y, c]).astype(jnp.int32)
    here = scal(x)
    lane = jnp.arange(128)
    cos_own, sin_own = turns((sp * 8 + tp) * 128 + lane)
    block = (y - jnp.arange(4)) % 4
    cos_q, sin_q = turns((sp * 1024 + block[:, None] * 256 + c * 128 + lane[None, :]).reshape(-1))

    def sends(arrays, perms):
        out = []
        for a, perm in zip(arrays, perms):
            out.append(send(a, perm))
        return out

    q_up = q_up.T
    kv_up_other, q_up_other = sends([kv_up, q_up], [CORE] * 2)
    normed, lat = kv_down_call(
        tokens, norm_gain[None], kv_down, rope_down.T, kv_gain[None], cos_own, sin_own
    )
    lats = [lat] + sends([lat] * 3, ALONG_Y[1:])
    q_lat = q_down_call(normed, q_down, q_gain.reshape(6, 128))
    q_lats = [q_lat] + sends([q_lat] * 3, ALONG_Y[1:])
    near, *moved = kv_up_call(here, lats, kv_up, kv_up_other)
    moved = sends(moved, ALONG_Z[1:])
    q0, *q_moved = q_up_call(here, q_lats, q_up, q_up_other, cos_q, sin_q)
    q_moved = sends(q_moved, ALONG_Z[1:])
    turn = [ALONG_X[1], ALONG_X[3], ALONG_X[2]]
    near = [near] + sends([near] * 3, turn)
    far = join_call(*moved)
    far = [far] + sends([far] * 3, turn)
    queries = join_call(q0, *q_moved)
    (other,) = sends([queries], [CORE])

    acc, qs = attention(here, near[0], far[0], (queries, other))
    for n, k in ((1, 1), (2, 3)):
        (acc,) = attention(scal((x - k) % 4), near[n], far[n], qs, acc)
    mine, theirs = attention(scal((x - 2) % 4), near[3], far[3], qs, acc, last=True)
    (theirs,) = sends([theirs], [CORE])
    result = merge_call(mine, theirs)
    ret = [result[0]] + sends(result[1:], [back(p) for p in ALONG_Z[1:]])
    parts = regroup_call(*ret)
    parts = [parts[0]] + sends(parts[1:], [back(p) for p in ALONG_Y[1:]])
    return out_call(here, parts, out_weight, out_gain[None])


def solution(mesh):
    return jax.shard_map(
        local,
        mesh=mesh,
        in_specs=(
            P(AXES, None),
            P(),
            P(),
            P(),
            P(),
            P(),
            P(),
            P(None, "tp"),
            P(None, "tp"),
            P(),
            P(),
        ),
        out_specs=P(AXES, None),
        check_vma=False,
    )
```
